32 devices in a mesh: sp: 4 (over z), fs: 4 (over y, x), tp: 2 (over core).
Axes of the slice: x: 2, y: 2, z: 4, core: 2. Of those that a mesh axis runs over, the one named last changes fastest.
Arguments:
- stream: bfloat16 [4, 4096, 2048], P('fs', 'sp', 'tp'), parts along dimension 0, may hold values from -6 to 6
- w_pool_in: bfloat16 [2048, 1024], P(None, 'tp'), may hold values from -0.125 to 0.125
- w_query: bfloat16 [2048, 1024], P(None, 'tp'), may hold values from -0.125 to 0.125
- w_forget: bfloat16 [2048, 1024], P(None, 'tp'), may hold values from -0.125 to 0.125
- w_value: bfloat16 [2048, 1024], P(None, 'tp'), may hold values from -0.125 to 0.125
- w_outgate: bfloat16 [2048, 1024], P(None, 'tp'), may hold values from -0.125 to 0.125
- pool_mix: bfloat16 [4, 256, 256], P('tp'), may hold values from -0.375 to 0.375
- pool_scale: float32 [1024], P('tp'), may hold values from 0.1 to 1.9
- lower_bound: float32 [1024], P('tp'), may hold values from 0.9 to 1
- extra_decay: float32 [4096, 8], P('sp', 'tp'), may hold values from -0.7 to 0
- rec_gain: float32 [128], replicated, may hold values from 0.1 to 1.9
- w_out_pool: bfloat16 [1024, 2048], P('tp'), may hold values from -0.125 to 0.125
- w_out_rec: bfloat16 [1024, 2048], P('tp'), may hold values from -0.125 to 0.125
- norm_gain: float32 [2048], P('tp'), may hold values from 0.1 to 1.9
- norm_bias: float32 [2048], P('tp'), may hold values from -3 to 3
Outputs:
- layer_out: bfloat16 [4, 4096, 2048], P('fs', 'sp', 'tp'), parts along dimension 0
The draws below stay inside these ranges and needn't reach their ends.
There are 4 independent parts, one for each index of `fs`. The reference program is written for one: setup_inputs(seed, part) draws one part's arguments, and reference() takes and returns one part's arrays. A program takes and returns all parts, laid end to end along the dimension named above; an argument that names none is the same for every part. Nothing has to cross between parts.
All inputs are finite; a program needn't handle non-finite values.
Results may differ from the reference program's by a relative error of at most 0.0085.
Values may be sent and summed in bfloat16 or wider, within the bound.
A program may use at most 128 MiB of HBM per device.

```python
import math
import jax
import jax.numpy as jnp
from jax import lax

D = 2048
POOL_W = 1024
REC_W = 1024
DK = 128
WMAX = 16
BLOCK_ROWS = 128
TOK_DEV = 1024
GROUP_CH = 256
HEADS = 8
SEQ = 4096


def draw_lower_bound(key, part):
    key_order = jax.random.fold_in(key, 11)
    key_fast = jax.random.fold_in(key, 12)
    key_slow = jax.random.fold_in(key, 13)
    order = jax.random.permutation(key_order, HEADS)
    chosen = order < HEADS // 2
    fast_gap = jnp.exp(jax.random.uniform(key_fast, (HEADS, DK), jnp.float32, math.log(0.03), math.log(0.06)))
    slow_gap = jnp.exp(jax.random.uniform(key_slow, (HEADS, DK), jnp.float32, math.log(0.16 / SEQ), math.log(0.8 / SEQ)))
    gaps = jnp.where(chosen[:, None], fast_gap, slow_gap)
    return (1.0 - gaps).reshape(REC_W).astype(jnp.float32)


def draw_extra_decay(key, part):
    key_base = jax.random.fold_in(key, 21)
    key_where = jax.random.fold_in(key, 22)
    key_drop = jax.random.fold_in(key, 23)
    blocks = SEQ // TOK_DEV
    base = jnp.exp(jax.random.uniform(key_base, (blocks,), jnp.float32, math.log(0.04 / SEQ), math.log(0.2 / SEQ)))
    base_rows = jnp.repeat(base, TOK_DEV)
    places = jax.random.randint(key_where, (2,), 0, SEQ)
    marked = jnp.any(jnp.arange(SEQ)[:, None] == places[None, :], axis=1)
    drops = jax.random.uniform(key_drop, (SEQ, HEADS), jnp.float32, 0.22, 0.69)
    total = base_rows[:, None] + jnp.where(marked[:, None], drops, jnp.float32(0.0))
    return (-total).astype(jnp.float32)


def shard_levels(rng, shape, split, least, largest):
    gain = 1.0
    for axis_at, parts in split:
        draws = jax.random.uniform(jax.random.fold_in(jax.random.fold_in(rng, 6), axis_at), (parts,), jnp.float32, least / len(split), largest / len(split))
        gain = gain * jnp.repeat(jnp.exp(draws), shape[axis_at] // parts).reshape((-1,) + (1,) * (len(shape) - 1 - axis_at))
    return gain


def normal_values(key, dims, width, bound, shards=(), dtype=jnp.bfloat16):
    factor_of = shard_levels(key, dims, shards, -0.22, 0.18) if shards else 1.0
    result = jax.random.normal(key, dims, jnp.float32) * width * factor_of
    return jnp.minimum(jnp.maximum(result, -bound), bound).astype(dtype)


def setup_inputs(seed: int = 0, part: int = 0) -> dict:
    key_list = jax.random.split(jax.random.key(seed), 16)
    own_keys = jax.random.split(jax.random.fold_in(key_list[15], part), 16)
    return {
        "stream": normal_values(own_keys[0], (1, SEQ, D), 1.0, 6.0, ((1, 4), (2, 2))),
        "w_pool_in": normal_values(key_list[1], (D, POOL_W), D ** -0.5, 0.125, ((1, 2),)),
        "w_query": normal_values(key_list[2], (D, REC_W), D ** -0.5, 0.125, ((1, 2),)),
        "w_forget": normal_values(key_list[3], (D, REC_W), D ** -0.5, 0.125, ((1, 2),)),
        "w_value": normal_values(key_list[4], (D, REC_W), D ** -0.5, 0.125, ((1, 2),)),
        "w_outgate": normal_values(key_list[5], (D, REC_W), D ** -0.5, 0.125, ((1, 2),)),
        "pool_mix": normal_values(key_list[6], (4, GROUP_CH, GROUP_CH), GROUP_CH ** -0.5, 0.375, ((0, 2),)),
        "pool_scale": jnp.clip(1.0 + 0.18 * jax.random.normal(key_list[7], (POOL_W,), jnp.float32), 0.1, 1.9),
        "lower_bound": draw_lower_bound(jax.random.fold_in(key_list[15], 71), part),
        "extra_decay": draw_extra_decay(jax.random.fold_in(key_list[15], 71), part),
        "rec_gain": jnp.clip(1.0 + 0.18 * jax.random.normal(key_list[10], (DK,), jnp.float32), 0.1, 1.9),
        "w_out_pool": normal_values(key_list[11], (POOL_W, D), (POOL_W + REC_W) ** -0.5, 0.125, ((0, 2),)),
        "w_out_rec": normal_values(key_list[12], (REC_W, D), (POOL_W + REC_W) ** -0.5, 0.125, ((0, 2),)),
        "norm_gain": jnp.clip(1.0 + 0.18 * jax.random.normal(key_list[13], (D,), jnp.float32), 0.1, 1.9),
        "norm_bias": normal_values(key_list[14], (D,), 0.5, 3.0, ((0, 2),), jnp.float32),
    }


ALPHA = 2.0 ** 0.25
EPS_RMS = 1e-06
EPS_NORM = 1e-05
HIGHEST = lax.Precision.HIGHEST

def pool_branch(pooled, pool_mix, pool_scale):
    length = pooled.shape[0]
    data = pooled.astype(jnp.float32)
    padded = jnp.pad(data, ((WMAX - 1, 0), (0, 0)))
    group_id = jnp.arange(POOL_W).astype(jnp.int32) // GROUP_CH
    window_len = jnp.left_shift(jnp.ones_like(group_id), group_id + 1)
    window_sum = jnp.zeros((length, POOL_W), jnp.float32)
    for lag_rows in range(WMAX):
        lagged = padded[WMAX - 1 - lag_rows:WMAX - 1 - lag_rows + length]
        window_sum = window_sum + jnp.where(lag_rows < window_len[None, :], lagged, jnp.float32(0.0))
    position = jnp.arange(1, length + 1).astype(jnp.float32)
    counts = jnp.minimum(position[:, None], window_len.astype(jnp.float32)[None, :])
    pool_diff = (window_sum / counts - data).astype(jnp.bfloat16)
    grouped = pool_diff.reshape(length, 4, GROUP_CH).astype(jnp.float32)
    mixed = jnp.einsum('tgc,gcd->tgd', grouped, pool_mix.astype(jnp.float32))
    return (mixed.reshape(length, POOL_W) * pool_scale).astype(jnp.bfloat16)

def recurrent_branch(queries, forget_in, value_in, gate_in, lower_bound, extra_decay, rec_gain):
    length = queries.shape[0]
    blocks = length // BLOCK_ROWS
    forget = lower_bound + (1.0 - lower_bound) * jax.nn.sigmoid(forget_in.astype(jnp.float32))
    log_keep = jnp.log(forget).reshape(length, HEADS, DK) + extra_decay[:, :, None]
    weight_in = (1.0 - forget).reshape(length, HEADS, DK)
    gated_query = jax.nn.silu(queries.astype(jnp.float32)).reshape(length, HEADS, DK)
    values = value_in.reshape(length, HEADS, DK)

    def to_blocks(arr):
        return arr.reshape(blocks, BLOCK_ROWS, HEADS, DK)
    lower_mask = jnp.tril(jnp.ones((BLOCK_ROWS, BLOCK_ROWS), jnp.float32))

    def block_step(state, inputs):
        query_blk, keep_blk, input_blk, value_blk = inputs
        value_wide = value_blk.astype(jnp.float32)
        log_total = jnp.cumsum(keep_blk, axis=0)
        query_up = query_blk * jnp.exp(log_total)
        input_down = input_blk * jnp.exp(-log_total)
        scores = jnp.einsum('thd,shd->hts', query_up, input_down, precision=HIGHEST) * lower_mask[None]
        scores = scores.astype(jnp.bfloat16).astype(jnp.float32)
        inside = jnp.einsum('hts,she->the', scores, value_wide, precision=HIGHEST)
        carried = jnp.einsum('thd,hde->the', query_up, state, precision=HIGHEST)
        log_end = log_total[-1]
        in_weight = (input_blk * jnp.exp(log_end[None] - log_total)).astype(jnp.bfloat16).astype(jnp.float32)
        new_state = jnp.exp(log_end)[:, :, None] * state + jnp.einsum('shd,she->hde', in_weight, value_wide, precision=HIGHEST)
        return (new_state, inside + carried)
    start_state = jnp.zeros((HEADS, DK, DK), jnp.float32)
    _, outputs = lax.scan(block_step, start_state, (to_blocks(gated_query), to_blocks(log_keep), to_blocks(weight_in), to_blocks(values)))
    rec_raw = outputs.reshape(length, HEADS, DK)
    rec_norm = rec_raw * lax.rsqrt(lax.optimization_barrier(jnp.mean(rec_raw * rec_raw, axis=-1, keepdims=True)) + EPS_RMS) * rec_gain
    gated = rec_norm * jax.nn.silu(gate_in.astype(jnp.float32)).reshape(length, HEADS, DK)
    return gated.reshape(length, REC_W).astype(jnp.bfloat16)

def reference(stream, w_pool_in, w_query, w_forget, w_value, w_outgate, pool_mix, pool_scale, lower_bound, extra_decay, rec_gain, w_out_pool, w_out_rec, norm_gain, norm_bias):
    features = stream[0]

    def project(weight):
        return jnp.dot(features, weight, preferred_element_type=jnp.float32).astype(jnp.bfloat16)
    pooled = project(w_pool_in)
    queries = project(w_query)
    forget_in = project(w_forget)
    value_in = project(w_value)
    gate_in = project(w_outgate)
    pool_out = pool_branch(pooled, pool_mix, pool_scale)
    rec_out = recurrent_branch(queries, forget_in, value_in, gate_in, lower_bound, extra_decay, rec_gain)
    mix = jnp.dot(pool_out, w_out_pool, preferred_element_type=jnp.float32) + jnp.dot(rec_out, w_out_rec, preferred_element_type=jnp.float32)
    resid = ALPHA * features.astype(jnp.float32) + mix
    row_mean = lax.optimization_barrier(jnp.mean(resid, axis=-1, keepdims=True))
    row_var = lax.optimization_barrier(jnp.mean((resid - row_mean) * (resid - row_mean), axis=-1, keepdims=True))
    normed = (resid - row_mean) * lax.rsqrt(row_var + EPS_NORM) * norm_gain + norm_bias
    return normed.astype(jnp.bfloat16)[None]
```

```python
import functools

import jax
import jax.numpy as jnp
from jax import lax
from jax.experimental import pallas as pl
from jax.experimental.pallas import tpu as pltpu
from jax.sharding import PartitionSpec as P

DK = 128
BLOCK_ROWS = 128
GROUP_CH = 256
HALO = 16
LANES = 128

ALPHA = 2.0**0.25
EPS_RMS = 1e-06
EPS_NORM = 1e-05
F32 = jnp.float32
BF16 = jnp.bfloat16
NT = (((1,), (1,)), ((), ()))
TN = (((0,), (0,)), ((), ()))


def dot(a, b, dims=None):
    if dims is None:
        return jnp.dot(a, b, preferred_element_type=F32)
    return lax.dot_general(a, b, dims, preferred_element_type=F32)


def half_sigmoid(x):
    return 0.5 + 0.5 * jnp.tanh(0.5 * x)


def mixer(
    n_sp, n_tp, rows_x,
    stream, w_pool, w_query, w_forget, w_value, w_gate,
    mix_in, scale_in, bound_in, extra_in, gain_in, wo_pool, wo_rec,
    out, stats,
    x_buf, w_buf, wo_buf, a_buf, v_buf, u_buf, e_buf, t_buf, p_buf, q_buf, g_buf, r_buf,
    o_buf, half_buf, state, state_out, state_in, halo_in, stat_own, stat_peer, stat_sum,
    mix, scale, bound, extra, gain,
    x_loc, x_send, x_recv, w_sem, wo_loc, wo_send, wo_recv, a_send, a_recv,
    st_send, st_recv, h_send, h_recv, s_send, s_recv, o_sem, t_sem, small_sem, met_sem, go_sem,
):
    sp, tp = lax.axis_index("sp"), lax.axis_index("tp")
    peer = 1 - tp
    length, feats = stream.shape[1], stream.shape[2]
    chans = bound.shape[1]
    heads = chans // DK
    pool_w = scale.shape[1]
    groups = mix.shape[0]
    chunks = length // rows_x
    blocks = length // BLOCK_ROWS
    per = rows_x // BLOCK_ROWS
    wide_x = 2 * rows_x
    wides, wide_per = length // wide_x, wide_x // BLOCK_ROWS

    def x_in(c):
        rows = pl.ds(c * rows_x, rows_x)
        return pltpu.make_async_copy(stream.at[0, rows], x_buf.at[tp, rows], x_loc.at[c])

    def x_out(c):
        rows = pl.ds(c * rows_x, rows_x)
        return pltpu.make_async_remote_copy(
            x_buf.at[tp, rows], x_buf.at[tp, rows], x_send.at[c], x_recv.at[c],
            device_id={"tp": peer}, device_id_type=pl.DeviceIdType.MESH)

    def w_in(i):
        src = (w_forget, w_value, w_pool, w_query, w_gate)[i]
        return [
            pltpu.make_async_copy(src.at[pl.ds(k * feats, feats)], w_buf.at[i, k], w_sem.at[i, k])
            for k in range(n_tp)
        ]

    my_cols = pl.ds(pl.multiple_of(tp * feats, LANES), feats)
    peer_cols = pl.ds(pl.multiple_of(peer * feats, LANES), feats)
    wo_places = ((wo_pool, pl.ds(0, pool_w)), (wo_rec, pl.ds(pool_w, chans)))

    def wo_in(i):
        src, place = wo_places[i]
        return pltpu.make_async_copy(src.at[:, my_cols], wo_buf.at[tp, place], wo_loc.at[i])

    def wo_out(i):
        src, place = wo_places[i]
        return pltpu.make_async_remote_copy(
            src.at[:, peer_cols], wo_buf.at[tp, place], wo_send.at[i], wo_recv.at[i],
            device_id={"tp": peer}, device_id_type=pl.DeviceIdType.MESH)

    def a_out(i, c):
        rows, cols = pl.ds(c * rows_x, rows_x), wo_places[i][1]
        return pltpu.make_async_remote_copy(
            a_buf.at[tp, rows, cols], a_buf.at[tp, rows, cols], a_send.at[i, c], a_recv.at[i, c],
            device_id={"tp": peer}, device_id_type=pl.DeviceIdType.MESH)

    def st_out(k, slot):
        return pltpu.make_async_remote_copy(
            state_out, state_in.at[slot], st_send.at[k], st_recv.at[slot],
            device_id={"sp": k}, device_id_type=pl.DeviceIdType.MESH)

    def h_out(k):
        return pltpu.make_async_remote_copy(
            p_buf.at[pl.ds(BLOCK_ROWS + length - HALO, HALO)], halo_in, h_send, h_recv,
            device_id={"sp": k}, device_id_type=pl.DeviceIdType.MESH)

    def s_out(c):
        return pltpu.make_async_remote_copy(
            stat_own.at[c], stat_peer.at[c], s_send.at[c], s_recv.at[c],
            device_id={"tp": peer}, device_id_type=pl.DeviceIdType.MESH)

    def o_out(c):
        rows = pl.ds(c * rows_x, rows_x)
        return pltpu.make_async_copy(o_buf.at[rows], out.at[rows], o_sem.at[c])

    def t_out(c):
        rows = pl.ds(c * rows_x, rows_x)
        return pltpu.make_async_copy(stat_sum.at[c], stats.at[rows], t_sem.at[c])

    smalls = [
        pltpu.make_async_copy(src, dst, small_sem.at[i])
        for i, (src, dst) in enumerate(
            ((bound_in, bound), (extra_in, extra), (mix_in, mix), (scale_in, scale), (gain_in, gain)))
    ]

    for c in range(chunks):
        x_in(c).start()
        if c == 0:
            for i in (0, 1):
                for copy in w_in(i):
                    copy.start()
            for copy in smalls:
                copy.start()

    barrier = pltpu.get_barrier_semaphore()

    @pl.when(tp > 0)
    def _():
        pl.semaphore_wait(barrier, 1)
        pl.semaphore_signal(met_sem, inc=1, device_id={"tp": peer}, device_id_type=pl.DeviceIdType.MESH)

    @pl.when(tp == 0)
    def _():
        pl.semaphore_signal(barrier, inc=1, device_id={"tp": peer}, device_id_type=pl.DeviceIdType.MESH)
        pl.semaphore_wait(met_sem, 1)

        def greet(k, _):
            pl.semaphore_signal(barrier, inc=1, device_id={"sp": k}, device_id_type=pl.DeviceIdType.MESH)
            return 0

        lax.fori_loop(0, sp, greet, 0)

    p_buf[pl.ds(0, BLOCK_ROWS), :] = jnp.zeros((BLOCK_ROWS, pool_w), BF16)
    state[...] = jnp.zeros_like(state)

    for c in range(chunks):
        x_in(c).wait()
        x_out(c).start()

    row_ids = lax.broadcasted_iota(jnp.int32, (BLOCK_ROWS, BLOCK_ROWS), 0)
    col_ids = lax.broadcasted_iota(jnp.int32, (BLOCK_ROWS, BLOCK_ROWS), 1)
    lower = row_ids >= col_ids
    tri = jnp.where(lower, 1.0, 0.0).astype(BF16)
    lower_twice = jnp.concatenate([row_ids, row_ids], axis=1) >= jnp.concatenate([col_ids, col_ids], axis=1)
    tri_twice = jnp.concatenate([tri, tri], axis=1)
    ones = jnp.ones((2 * BLOCK_ROWS, DK), BF16)

    for i in (0, 1):
        for copy in w_in(i):
            copy.wait()
    for copy in smalls:
        copy.wait()
    for i in (2, 3, 4):
        for copy in w_in(i):
            copy.start()
    for i in range(2):
        wo_in(i).start()
        wo_out(i).start()

    def first(c, _):
        rows = pl.ds(pl.multiple_of(c * wide_x, wide_x), wide_x)
        own = x_buf[tp, rows]
        f_own = dot(own, w_buf[0, tp])
        v_own = dot(own, w_buf[1, tp])
        for k in range(2):
            x_out(2 * c + k).wait_recv()
        other = x_buf[peer, rows]
        f_in = (f_own + dot(other, w_buf[0, peer])).astype(BF16).astype(F32)
        vals = (v_own + dot(other, w_buf[1, peer])).astype(BF16)
        v_buf[rows, :] = vals
        open_part = 1.0 - bound[...]
        for j in range(wide_per):
            part = slice(j * BLOCK_ROWS, (j + 1) * BLOCK_ROWS)
            b = c * wide_per + j
            brows = pl.ds(pl.multiple_of(b * BLOCK_ROWS, BLOCK_ROWS), BLOCK_ROWS)
            weight = open_part * (0.5 - 0.5 * jnp.tanh(0.5 * f_in[part]))
            keep = jnp.log(1.0 - weight)
            high = keep.astype(BF16)
            low = (keep - high.astype(F32)).astype(BF16)
            drop = extra[:, brows]
            drop_high = drop.astype(BF16).astype(F32)
            drop_low = drop - drop_high
            drops = []
            for h in range(heads):
                pair = jnp.concatenate([drop_high[h:h + 1], drop_low[h:h + 1]], axis=1)
                wide = jnp.where(lower_twice, jnp.broadcast_to(pair, (BLOCK_ROWS, 2 * BLOCK_ROWS)), 0.0)
                drops.append(dot(wide.astype(BF16), ones))
            total = dot(tri_twice, jnp.concatenate([high, low], axis=0)) + jnp.concatenate(drops, axis=1)
            middle = 0.5 * total[BLOCK_ROWS - 1:BLOCK_ROWS]
            e_buf[brows, :] = jnp.exp(total - middle)
            down = (weight * jnp.exp(middle - total)).astype(BF16)
            u_buf[brows, :] = down
            half = jnp.exp(middle)
            half_buf[b] = jnp.broadcast_to(half, (8, chans))
            for h in range(heads):
                lanes = slice(h * DK, (h + 1) * DK)
                hh = half[:, lanes]
                term = dot(vals[part, lanes], down[:, lanes], TN) * hh
                t_buf[b, :, lanes] = term
                state[:, lanes] = hh * hh * state[:, lanes] + term
        return 0

    lax.fori_loop(0, wides, first, 0)

    for copy in w_in(2):
        copy.wait()

    def second(c, _):
        start = c * rows_x if isinstance(c, int) else pl.multiple_of(c * rows_x, rows_x)
        rows = pl.ds(start, rows_x)
        pooled = dot(x_buf[tp, rows], w_buf[2, tp]) + dot(x_buf[peer, rows], w_buf[2, peer])
        p_buf[pl.ds(start + BLOCK_ROWS, rows_x), :] = pooled.astype(BF16)
        return 0

    second(chunks - 1, 0)

    @pl.when((tp == 0) & (sp + 1 < n_sp))
    def _():
        pl.semaphore_wait(barrier, n_sp - 1 - sp)
        pl.semaphore_signal(go_sem, inc=1, device_id={"tp": peer}, device_id_type=pl.DeviceIdType.MESH)

    @pl.when((tp > 0) & (sp + 1 < n_sp))
    def _():
        pl.semaphore_wait(go_sem, 1)

    @pl.when(sp + 1 < n_sp)
    def _():
        h_out(sp + 1).start()

    log_half = half_buf[0, 0:1]
    for b in range(1, blocks):
        log_half = log_half * half_buf[b, 0:1]
    state_out[pl.ds(0, DK), :] = state[...].astype(BF16)
    state_out[pl.ds(DK, HALO), :] = jnp.broadcast_to(log_half * log_half, (HALO, chans)).astype(BF16)

    def send_state(k, _):
        st_out(k, sp).start()
        return 0

    lax.fori_loop(sp + 1, n_sp, send_state, 0)

    lax.fori_loop(0, chunks - 1, second, 0)

    for i in (3, 4):
        for copy in w_in(i):
            copy.wait()

    wide_rows = lax.broadcasted_iota(jnp.int32, (BLOCK_ROWS, 2 * BLOCK_ROWS), 0) + BLOCK_ROWS
    wide_cols = lax.broadcasted_iota(jnp.int32, (BLOCK_ROWS, 2 * BLOCK_ROWS), 1)
    back = wide_rows - wide_cols
    count = lax.broadcasted_iota(jnp.int32, (BLOCK_ROWS, LANES), 0) + (sp * length + 1)

    def third(step, _):
        c = wides - 1 - step

        @pl.when((step == wides - 1) & (sp > 0))
        def _():
            h_out(sp).wait_recv()
            p_buf[pl.ds(BLOCK_ROWS - HALO, HALO), :] = halo_in[...]

        rows = pl.ds(pl.multiple_of(c * wide_x, wide_x), wide_x)
        own, other = x_buf[tp, rows], x_buf[peer, rows]
        q_in = (dot(own, w_buf[3, tp]) + dot(other, w_buf[3, peer])).astype(BF16).astype(F32)
        ups = (q_in * half_sigmoid(q_in) * e_buf[rows, :]).astype(BF16)
        q_buf[rows, :] = ups
        g_in = dot(own, w_buf[4, tp]) + dot(other, w_buf[4, peer])
        g_buf[rows, :] = g_in.astype(BF16)
        for k in range(wide_per):
            start = pl.multiple_of(c * wide_x + k * BLOCK_ROWS, BLOCK_ROWS)
            brows = pl.ds(start, BLOCK_ROWS)
            near = p_buf[pl.ds(start, 2 * BLOCK_ROWS), :]
            for j in range(groups):
                lanes = slice(j * GROUP_CH, (j + 1) * GROUP_CH)
                window = jnp.left_shift(jnp.int32(2), tp * groups + j)
                band = jnp.where((back >= 0) & (back < window), 1.0, 0.0).astype(BF16)
                share = 1.0 / jnp.minimum(count + start, window).astype(F32)
                share = jnp.concatenate([share] * (GROUP_CH // LANES), axis=1)
                sums = dot(band, near[:, lanes])
                diff = (sums * share - near[BLOCK_ROWS:, lanes].astype(F32)).astype(BF16)
                a_buf[tp, brows, lanes] = (dot(diff, mix[j]) * scale[:, lanes]).astype(BF16)
            for h in range(heads):
                lanes = slice(h * DK, (h + 1) * DK)
                up = ups[k * BLOCK_ROWS:(k + 1) * BLOCK_ROWS, lanes]
                scores = jnp.where(lower, dot(up, u_buf[brows, lanes], NT), 0.0).astype(BF16)
                e_buf[brows, lanes] = dot(scores, v_buf[brows, lanes])
        for k in range(2):
            a_out(0, 2 * c + k).start()
        return 0

    lax.fori_loop(0, wides, third, 0)

    for i in range(2):
        wo_in(i).wait()
        wo_out(i).wait_recv()

    pool_at, rec_at = wo_places[0][1], wo_places[1][1]

    def pool_part(step, _):
        c = chunks - 1 - step
        rows = pl.ds(pl.multiple_of(c * rows_x, rows_x), rows_x)
        mine = dot(a_buf[tp, rows, pool_at], wo_buf[tp, pool_at]) + ALPHA * x_buf[tp, rows].astype(F32)
        a_out(0, c).wait_recv()
        r_buf[rows, :] = mine + dot(a_buf[peer, rows, pool_at], wo_buf[peer, pool_at])
        return 0

    lax.fori_loop(0, chunks, pool_part, 0)

    state[...] = jnp.zeros_like(state)

    def join(k, _):
        st_out(sp, k).wait_recv()
        keep = state_in[k, pl.ds(DK, HALO), :].astype(F32)[0:1]
        state[...] = keep * state[...] + state_in[k, pl.ds(0, DK), :].astype(F32)
        return 0

    lax.fori_loop(0, sp, join, 0)

    def fourth(c, _):
        for k in range(per):
            b = c * per + k
            rows = pl.ds(pl.multiple_of(b * BLOCK_ROWS, BLOCK_ROWS), BLOCK_ROWS)
            half = half_buf[b, 0:1]
            before = state[...] * half
            carried = before.astype(BF16)
            state[...] = before * half + t_buf[b]
            for h in range(heads):
                lanes = slice(h * DK, (h + 1) * DK)
                raw = e_buf[rows, lanes] + dot(q_buf[rows, lanes], carried[:, lanes], NT)
                power = jnp.mean(raw * raw, axis=-1, keepdims=True)
                gate = g_buf[rows, lanes].astype(F32)
                rec = raw * lax.rsqrt(power + EPS_RMS) * gain[...] * (gate * half_sigmoid(gate))
                a_buf[tp, rows, pool_w + h * DK:pool_w + (h + 1) * DK] = rec.astype(BF16)
        a_out(1, c).start()
        return 0

    lax.fori_loop(0, chunks, fourth, 0)

    def fold(x):
        acc = x[:, :LANES]
        for k in range(1, feats // LANES):
            acc = acc + x[:, k * LANES:(k + 1) * LANES]
        return acc

    first_half = lax.broadcasted_iota(jnp.int32, (rows_x, LANES), 1) < LANES // 2

    def fifth(c, _):
        rows = pl.ds(pl.multiple_of(c * rows_x, rows_x), rows_x)
        mine = r_buf[rows, :] + dot(a_buf[tp, rows, rec_at], wo_buf[tp, rec_at])
        a_out(1, c).wait_recv()
        resid = mine + dot(a_buf[peer, rows, rec_at], wo_buf[peer, rec_at])
        o_buf[rows, :] = resid.astype(BF16)
        sums, squares = fold(resid), fold(resid * resid)
        sums = sums + pltpu.roll(sums, LANES // 2, 1)
        squares = squares + pltpu.roll(squares, LANES // 2, 1)
        stat_own[c] = jnp.where(first_half, sums, squares)
        s_out(c).start()
        o_out(c).start()
        return 0

    lax.fori_loop(0, chunks, fifth, 0)

    for c in range(chunks):
        s_out(c).wait_recv()
        stat_sum[c] = stat_own[c] + stat_peer[c]
        t_out(c).start()

    for c in range(chunks):
        x_out(c).wait_send()
        s_out(c).wait_send()
        o_out(c).wait()
        t_out(c).wait()
        for i in range(2):
            a_out(i, c).wait_send()
    for i in range(2):
        wo_out(i).wait_send()

    def sent_state(k, _):
        st_out(k, sp).wait_send()
        return 0

    lax.fori_loop(sp + 1, n_sp, sent_state, 0)

    @pl.when(sp + 1 < n_sp)
    def _():
        h_out(sp + 1).wait_send()


def finish(width, rows, resid, stats, norm_gain, norm_bias, out,
           r_buf, s_buf, o_buf, gain, bias, r_sem, s_sem, o_sem, n_sem):
    pieces = resid.shape[0] // rows

    def copies(c):
        part = pl.ds(c * rows, rows)
        return (
            pltpu.make_async_copy(stats.at[part], s_buf.at[part], s_sem.at[c]),
            pltpu.make_async_copy(resid.at[part], r_buf.at[part], r_sem.at[c]),
            pltpu.make_async_copy(o_buf.at[part], out.at[0, part], o_sem.at[c]),
        )

    norms = (
        pltpu.make_async_copy(norm_gain, gain, n_sem.at[0]),
        pltpu.make_async_copy(norm_bias, bias, n_sem.at[1]),
    )
    for copy in norms:
        copy.start()
    for c in range(pieces):
        for copy in copies(c)[:2]:
            copy.start()
    for copy in norms:
        copy.wait()
    first_half = lax.broadcasted_iota(jnp.int32, (rows, LANES), 1) < LANES // 2
    for c in range(pieces):
        part = pl.ds(c * rows, rows)
        for copy in copies(c)[:2]:
            copy.wait()
        both = s_buf[part, :]
        mean = jnp.sum(jnp.where(first_half, both, 0.0), axis=1, keepdims=True) / width
        square = jnp.sum(jnp.where(first_half, 0.0, both), axis=1, keepdims=True) / width
        inv = lax.rsqrt(square - mean * mean + EPS_NORM)
        o_buf[part, :] = ((r_buf[part, :].astype(F32) - mean) * inv * gain[...] + bias[...]).astype(BF16)
        copies(c)[2].start()
    for c in range(pieces):
        copies(c)[2].wait()


def solution(mesh):
    n_sp, n_tp = mesh.shape["sp"], mesh.shape["tp"]

    def local(stream, w_pool, w_query, w_forget, w_value, w_gate, mix, scale, bound, extra,
              gain, wo_pool, wo_rec, norm_gain, norm_bias):
        length, feats = stream.shape[1], stream.shape[2]
        chans, pool_w = bound.shape[0], scale.shape[0]
        blocks = length // BLOCK_ROWS
        rows_x = 256
        chunks = length // rows_x
        hbm = pl.BlockSpec(memory_space=pl.ANY)
        dma = pltpu.SemaphoreType.DMA
        scratch = [
            pltpu.VMEM((n_tp, length, feats), BF16),
            pltpu.VMEM((5, n_tp, feats, chans), BF16),
            pltpu.VMEM((n_tp, pool_w + chans, feats), BF16),
            pltpu.VMEM((n_tp, length, pool_w + chans), BF16),
            pltpu.VMEM((length, chans), BF16),
            pltpu.VMEM((length, chans), BF16),
            pltpu.VMEM((length, chans), F32),
            pltpu.VMEM((blocks, DK, chans), F32),
            pltpu.VMEM((BLOCK_ROWS + length, pool_w), BF16),
            pltpu.VMEM((length, chans), BF16),
            pltpu.VMEM((length, chans), BF16),
            pltpu.VMEM((length, feats), F32),
            pltpu.VMEM((length, feats), BF16),
            pltpu.VMEM((blocks, 8, chans), F32),
            pltpu.VMEM((DK, chans), F32),
            pltpu.VMEM((DK + HALO, chans), BF16),
            pltpu.VMEM((n_sp, DK + HALO, chans), BF16),
            pltpu.VMEM((HALO, pool_w), BF16),
            pltpu.VMEM((chunks, rows_x, LANES), F32),
            pltpu.VMEM((chunks, rows_x, LANES), F32),
            pltpu.VMEM((chunks, rows_x, LANES), F32),
            pltpu.VMEM(mix.shape, BF16),
            pltpu.VMEM((1, pool_w), F32),
            pltpu.VMEM((1, chans), F32),
            pltpu.VMEM((chans // DK, length), F32),
            pltpu.VMEM((1, DK), F32),
            dma((chunks,)), dma((chunks,)), dma((chunks,)), dma((5, n_tp)),
            dma((2,)), dma((2,)), dma((2,)), dma((2, chunks)), dma((2, chunks)),
            dma((n_sp,)), dma((n_sp,)), dma, dma, dma((chunks,)), dma((chunks,)), dma((chunks,)),
            dma((chunks,)), dma((5,)), pltpu.SemaphoreType.REGULAR, pltpu.SemaphoreType.REGULAR,
        ]
        row = lambda x: x.reshape(1, -1)
        resid, stats = pl.pallas_call(
            functools.partial(mixer, n_sp, n_tp, rows_x),
            out_shape=(
                jax.ShapeDtypeStruct((length, feats), BF16), jax.ShapeDtypeStruct((length, LANES), F32)),
            in_specs=[hbm] * 13,
            out_specs=(hbm, hbm),
            scratch_shapes=scratch,
            compiler_params=pltpu.CompilerParams(
                collective_id=0, has_side_effects=True, vmem_limit_bytes=60 * 1024 * 1024),
            name="mixer",
        )(stream, w_pool, w_query, w_forget, w_value, w_gate, mix, row(scale), row(bound), extra.T,
          row(gain), wo_pool, wo_rec)
        piece = 128
        pieces = length // piece
        return pl.pallas_call(
            functools.partial(finish, n_tp * feats, piece),
            out_shape=jax.ShapeDtypeStruct(stream.shape, BF16),
            in_specs=[hbm] * 4,
            out_specs=hbm,
            scratch_shapes=[
                pltpu.VMEM((length, feats), BF16),
                pltpu.VMEM((length, LANES), F32),
                pltpu.VMEM((length, feats), BF16),
                pltpu.VMEM((1, feats), F32),
                pltpu.VMEM((1, feats), F32),
                dma((pieces,)), dma((pieces,)), dma((pieces,)), dma((2,)),
            ],
            compiler_params=pltpu.CompilerParams(vmem_limit_bytes=60 * 1024 * 1024),
            name="finish",
        )(resid, stats, row(norm_gain), row(norm_bias))

    placed = (
        P("fs", "sp", "tp"), P(None, "tp"), P(None, "tp"), P(None, "tp"), P(None, "tp"),
        P(None, "tp"), P("tp", None, None), P("tp"), P("tp"), P("sp", "tp"), P(),
        P("tp", None), P("tp", None), P("tp"), P("tp"),
    )
    return jax.shard_map(
        local, mesh=mesh, in_specs=placed, out_specs=P("fs", "sp", "tp"), check_vma=False
    )
```

```python
import functools

import jax
import jax.numpy as jnp
from jax import lax
from jax.experimental import pallas as pl
from jax.experimental.pallas import tpu as pltpu
from jax.sharding import PartitionSpec as P

DK = 128
BLOCK_ROWS = 128
GROUP_CH = 256
HALO = 16
LANES = 128
ROWS = 256

ALPHA = 2.0**0.25
EPS_RMS = 1e-06
EPS_NORM = 1e-05
F32 = jnp.float32
BF16 = jnp.bfloat16
NT = (((1,), (1,)), ((), ()))
TN = (((0,), (0,)), ((), ()))
MESH = pl.DeviceIdType.MESH


def dot(a, b, dims=None):
    if dims is None:
        return jnp.dot(a, b, preferred_element_type=F32)
    return lax.dot_general(a, b, dims, preferred_element_type=F32)


def half_sigmoid(x):
    return 0.5 + 0.5 * jnp.tanh(0.5 * x)


def skew(items, stages, lag=1):
    items, count = list(items), 0
    order = []
    for t in range(len(items) + lag * (stages - 1)):
        for stage in reversed(range(stages)):
            if 0 <= t - stage * lag < len(items):
                order.append(t - stage * lag)
                count += 1

    def run():
        for i in order:
            next(items[i], None)
            yield

    return count, run()


def weave(bigs, smalls):
    n_big, n_small = (sum(n for n, _ in steps) for steps in (bigs, smalls))
    rest = [step for _, steps in smalls for step in [steps]]
    small = (None for steps in rest for _ in steps)
    done = 0
    for i, _ in enumerate(piece for _, steps in bigs for piece in steps):
        want = -(-(i + 1) * n_small // n_big)
        while done < want:
            next(small, None)
            done += 1
    for _ in small:
        pass


def mixer(
    n_sp, n_tp,
    stream, w_pool, w_query, w_forget, w_value, w_gate,
    mix_in, scale_in, bound_in, extra_in, gain_in, wo_pool, wo_rec, norm_gain_in, norm_bias_in,
    out,
    x_own, x_peer, w_buf, wo_own, wo_peer, a_own, a_peer, f_buf, v_buf, u_buf, e_buf, t_buf, p_buf, q_buf, sq_buf, g_buf, r_buf,
    o_buf, half_buf, state, state_out, state_in, halo_in, stat_own, stat_peer, norm_gain, norm_bias,
    mix, scale, bound, extra, extra_t, gain,
    x_loc, x_send, x_recv, w_sem, wo_loc, wo_send, wo_recv, a_send, a_recv,
    st_send, st_recv, h_send, h_recv, s_send, s_recv, o_sem, small_sem, met_sem, go_sem,
):
    sp, tp = lax.axis_index("sp"), lax.axis_index("tp")
    peer = 1 - tp
    length, feats = stream.shape[1], stream.shape[2]
    chans = bound.shape[1]
    heads = chans // DK
    pool_w = scale.shape[1]
    groups = mix.shape[0]
    chunks = length // ROWS
    blocks = length // BLOCK_ROWS
    per = ROWS // BLOCK_ROWS
    pair = 2 * DK

    def rows_of(c, size=ROWS, base=0):
        start = c * size + base
        return pl.ds(start if isinstance(start, int) else pl.multiple_of(start, BLOCK_ROWS), size)

    def x_in(c):
        rows = rows_of(c)
        return pltpu.make_async_copy(stream.at[0, rows], x_own.at[rows], x_loc.at[c])

    def x_out(c):
        rows = rows_of(c)
        return pltpu.make_async_remote_copy(
            x_own.at[rows], x_peer.at[rows], x_send.at[c], x_recv.at[c],
            device_id={"tp": peer}, device_id_type=MESH)

    def w_in(i, k):
        src = (w_forget, w_value, w_pool, w_query, w_gate)[i]
        rows = pl.ds(pl.multiple_of((tp, peer)[k] * feats, LANES), feats)
        return pltpu.make_async_copy(src.at[rows], w_buf.at[i, k], w_sem.at[i, k])

    my_cols = pl.ds(pl.multiple_of(tp * feats, LANES), feats)
    peer_cols = pl.ds(pl.multiple_of(peer * feats, LANES), feats)
    wo_places = ((wo_pool, pl.ds(0, pool_w)), (wo_rec, pl.ds(pool_w, chans)))

    def wo_in(i):
        src, place = wo_places[i]
        return pltpu.make_async_copy(src.at[:, my_cols], wo_own.at[place], wo_loc.at[i])

    def wo_out(i):
        src, place = wo_places[i]
        return pltpu.make_async_remote_copy(
            src.at[:, peer_cols], wo_peer.at[place], wo_send.at[i], wo_recv.at[i],
            device_id={"tp": peer}, device_id_type=MESH)

    def a_out(i, c):
        rows, cols = rows_of(c), wo_places[i][1]
        return pltpu.make_async_remote_copy(
            a_own.at[rows, cols], a_peer.at[rows, cols], a_send.at[i, c], a_recv.at[i, c],
            device_id={"tp": peer}, device_id_type=MESH)

    def st_out(pr):
        return pltpu.make_async_remote_copy(
            state_out.at[pr], state_in.at[pr], st_send.at[pr], st_recv.at[pr],
            device_id={"sp": lax.rem(sp + 1, n_sp)}, device_id_type=MESH)

    def h_out(k):
        return pltpu.make_async_remote_copy(
            p_buf.at[pl.ds(BLOCK_ROWS + length - HALO, HALO)], halo_in, h_send, h_recv,
            device_id={"sp": k}, device_id_type=MESH)

    def s_out(c):
        return pltpu.make_async_remote_copy(
            stat_own.at[c], stat_peer.at[c], s_send.at[c], s_recv.at[c],
            device_id={"tp": peer}, device_id_type=MESH)

    def o_out(c):
        rows = rows_of(c)
        return pltpu.make_async_copy(o_buf.at[rows], out.at[rows], o_sem.at[c])

    smalls = [
        pltpu.make_async_copy(src, dst, small_sem.at[i])
        for i, (src, dst) in enumerate(
            ((bound_in, bound), (extra_in, extra), (mix_in, mix), (scale_in, scale), (gain_in, gain),
             (norm_gain_in, norm_gain), (norm_bias_in, norm_bias)))
    ]

    barrier = pltpu.get_barrier_semaphore()

    @pl.when(tp == 0)
    def _():
        pl.semaphore_signal(barrier, inc=1, device_id={"tp": peer}, device_id_type=MESH)

    x_in(0).start()
    w_in(0, 0).start()
    for c in range(1, chunks):
        x_in(c).start()
    w_in(1, 0).start()
    for copy in smalls:
        copy.start()

    @pl.when(tp > 0)
    def _():
        pl.semaphore_wait(barrier, 1)
        pl.semaphore_signal(met_sem, inc=1, device_id={"tp": peer}, device_id_type=MESH)

    @pl.when(tp == 0)
    def _():
        pl.semaphore_wait(met_sem, 1)

    @pl.when((tp == 0) & (sp > 0))
    def _():
        pl.semaphore_signal(barrier, inc=1, device_id={"sp": lax.rem(sp + n_sp - 1, n_sp)}, device_id_type=MESH)

    p_buf[pl.ds(0, BLOCK_ROWS), :] = jnp.zeros((BLOCK_ROWS, pool_w), BF16)
    state[...] = jnp.zeros_like(state)

    row_ids = lax.broadcasted_iota(jnp.int32, (BLOCK_ROWS, BLOCK_ROWS), 0)
    col_ids = lax.broadcasted_iota(jnp.int32, (BLOCK_ROWS, BLOCK_ROWS), 1)
    lower = row_ids >= col_ids
    tri = jnp.where(lower, 1.0, 0.0).astype(BF16)
    tri_twice = jnp.concatenate([tri, tri], axis=1)

    def own_fv(c, i):
        rows = rows_of(c)
        r_buf[rows, i * chans:(i + 1) * chans] = dot(x_own[rows], w_buf[i, 0])

    def peer_fv(c, pr):
        rows = rows_of(c)
        cols = slice(pr * pair, (pr + 1) * pair)
        parts = [dot(x_peer[rows], w_buf[i, 1, :, cols]) for i in range(2)]
        for i, buf in ((0, f_buf), (1, v_buf)):
            both = slice(i * chans + pr * pair, i * chans + (pr + 1) * pair)
            buf[rows, cols] = (r_buf[rows, both] + parts[i]).astype(BF16)
        yield

    def project(c, i, buf, base=0):
        rows = rows_of(c)
        part = dot(x_own[rows], w_buf[i, 0])
        yield
        buf[rows_of(c, ROWS, base), :] = (part + dot(x_peer[rows], w_buf[i, 1])).astype(BF16)
        yield

    def gate_one(b, pr):
        brows = rows_of(b, BLOCK_ROWS)
        lanes = slice(pr * pair, (pr + 1) * pair)
        tile = BLOCK_ROWS // 4
        tiles = [slice(b * BLOCK_ROWS + k * tile, b * BLOCK_ROWS + (k + 1) * tile) for k in range(4)]
        weights, highs, lows = [], [], []
        for part in tiles:
            f_in = f_buf[part, lanes].astype(F32)
            drop = jnp.concatenate(
                [jnp.broadcast_to(extra_t[part, h:h + 1], (tile, DK)) for h in (2 * pr, 2 * pr + 1)], axis=1)
            weight = (1.0 - bound[:, lanes]) * (0.5 - 0.5 * jnp.tanh(0.5 * f_in))
            keep = jnp.log(1.0 - weight) + drop
            high = keep.astype(BF16)
            highs.append(high)
            lows.append((keep - high.astype(F32)).astype(BF16))
            e_buf[part, lanes] = weight
        total = dot(tri_twice, jnp.concatenate(highs + lows, axis=0))
        yield
        middle = 0.5 * total[BLOCK_ROWS - 1:BLOCK_ROWS]
        half = jnp.exp(middle)
        half_buf[b, :, lanes] = jnp.broadcast_to(half, (8, pair))
        downs = []
        for k, part in enumerate(tiles):
            apart = total[k * tile:(k + 1) * tile] - middle
            down = (e_buf[part, lanes] * jnp.exp(-apart)).astype(BF16)
            downs.append(down)
            u_buf[part, lanes] = down
            e_buf[part, lanes] = jnp.exp(apart)
        down = jnp.concatenate(downs, axis=0)
        terms = [
            dot(v_buf[brows, pr * pair + j * DK:pr * pair + (j + 1) * DK], down[:, j * DK:(j + 1) * DK], TN)
            for j in range(2)]
        yield
        term = jnp.concatenate(terms, axis=1) * half
        t_buf[b, :, lanes] = term
        state[:, lanes] = half * half * state[:, lanes] + term
        yield

    def gates(c, pr):
        return skew([gate_one(c * per + k, pr) for k in range(per)], 3)

    back = (lax.broadcasted_iota(jnp.int32, (BLOCK_ROWS, 2 * BLOCK_ROWS), 0) + BLOCK_ROWS
            - lax.broadcasted_iota(jnp.int32, (BLOCK_ROWS, 2 * BLOCK_ROWS), 1))
    count = lax.broadcasted_iota(jnp.int32, (BLOCK_ROWS, LANES), 0) + (sp * length + 1)

    def pool_one(b, j):
        start = b * BLOCK_ROWS
        brows = rows_of(b, BLOCK_ROWS)
        lanes = slice(j * GROUP_CH, (j + 1) * GROUP_CH)
        near = p_buf[rows_of(b, BLOCK_ROWS, 0), lanes]
        here = p_buf[rows_of(b, BLOCK_ROWS, BLOCK_ROWS), lanes]
        window = jnp.left_shift(jnp.int32(2), tp * groups + j)
        band = jnp.where((back >= 0) & (back < window), 1.0, 0.0).astype(BF16)
        sums = dot(band, jnp.concatenate([near, here], axis=0))
        yield
        share = 1.0 / jnp.minimum(count + start, window).astype(F32)
        share = jnp.concatenate([share] * (GROUP_CH // LANES), axis=1)
        diff = (sums * share - here.astype(F32)).astype(BF16)
        mixed = dot(diff, mix[j])
        yield
        a_own[brows, lanes] = (mixed * scale[:, lanes]).astype(BF16)
        yield

    def pools(c):
        return skew([pool_one(c * per + k, j) for k in range(per) for j in range(groups)], 3)

    def score_one(b, h):
        brows = rows_of(b, BLOCK_ROWS)
        lanes = slice(h * DK, (h + 1) * DK)
        q_in = q_buf[brows, lanes].astype(F32)
        up = (q_in * half_sigmoid(q_in) * e_buf[brows, lanes]).astype(BF16)
        sq_buf[brows, h * pair + DK:(h + 1) * pair] = up
        tile = dot(up, u_buf[brows, lanes], NT)
        yield
        sq_buf[brows, h * pair:h * pair + DK] = jnp.where(lower, tile, 0.0).astype(BF16)
        yield

    def scores(c):
        return skew([score_one(c * per + k, h) for k in range(per) for h in range(heads)], 2, 2)

    def mix_one(b, h):
        brows = rows_of(b, BLOCK_ROWS)
        lanes = slice(h * DK, (h + 1) * DK)
        half = half_buf[b, 0:1, lanes]
        before = state[:, lanes] * half
        state[:, lanes] = before * half + t_buf[b, :, lanes]
        carried = jnp.transpose(before.astype(BF16))
        yield
        raw = dot(sq_buf[brows, h * pair:(h + 1) * pair],
                  jnp.concatenate([v_buf[brows, lanes], carried], axis=0))
        yield
        power = jnp.mean(raw * raw, axis=-1, keepdims=True)
        yield
        gate = g_buf[brows, lanes].astype(F32)
        rec = raw * lax.rsqrt(power + EPS_RMS) * gain[...] * (gate * half_sigmoid(gate))
        a_own[brows, pool_w + h * DK:pool_w + (h + 1) * DK] = rec.astype(BF16)
        yield

    def mixes(c):
        return skew([mix_one(c * per + k, h) for k in range(per) for h in range(heads)], 4)

    with jax.named_scope("own_fv"):
        for c in range(chunks):
            if c < 2:
                for d in range(1) if c == 0 else range(1, chunks):
                    x_in(d).wait()
                    x_out(d).start()
            if c == 0:
                w_in(0, 0).wait()
                for i in range(2):
                    w_in(i, 1).start()
            own_fv(c, 0)
        w_in(1, 0).wait()
        for copy in smalls:
            copy.wait()
        for b in range(blocks):
            brows = rows_of(b, BLOCK_ROWS)
            extra_t[brows, 0:heads] = jnp.transpose(extra[:, brows])
        for c in range(chunks):
            own_fv(c, 1)

    for i in (2, 3, 4):
        for k in range(n_tp):
            w_in(i, k).start()
    for i in range(2):
        wo_in(i).start()
        wo_out(i).start()

    more = sp + 1 < n_sp

    def own_state(pr):
        @pl.when((sp == 0) & more)
        def _():
            state_out[pr] = state[:, pr * pair:(pr + 1) * pair].astype(BF16)
            st_out(pr).start()

    def next_state(pr, here):
        @pl.when(here & (sp > 0) & more)
        def _():
            lanes = slice(pr * pair, (pr + 1) * pair)
            root = half_buf[0, 0:1, lanes]
            for b in range(1, blocks):
                root = root * half_buf[b, 0:1, lanes]
            st_out(pr).wait_recv()
            state_out[pr] = (root * root * state_in[pr].astype(F32) + state[:, lanes]).astype(BF16)
            st_out(pr).start()

    fv_steps = [(c, pr) for pr in range(heads // 2) for c in range(chunks)]
    gate_items = [gate_one(b, pr) for pr in range(heads // 2) for b in range(blocks)]

    def fv_step(k):
        if k >= len(fv_steps):
            for _ in project(chunks - 1, 2, p_buf, BLOCK_ROWS):
                pass
            return
        c, pr = fv_steps[k]
        if pr == 0 and c % 2 == 0:
            for d in (c, c + 1):
                x_out(d).wait_recv()
        for _ in peer_fv(c, pr):
            pass

    def gate_slot(t):
        for stage in (2, 1, 0):
            if 0 <= t - stage < len(gate_items):
                next(gate_items[t - stage], None)

    for i in range(2):
        w_in(i, 1).wait()
    with jax.named_scope("fv"):
        fv_step(0)
        fv_step(1)
        for t in range(blocks + 2):
            if t % per == 0:
                fv_step(2 + t // per)
            gate_slot(t)

    with jax.named_scope("greet_wait"):
        @pl.when((tp == 0) & more)
        def _():
            pl.semaphore_wait(barrier, 1)
            pl.semaphore_signal(go_sem, inc=1, device_id={"tp": peer}, device_id_type=MESH)

        @pl.when((tp > 0) & more)
        def _():
            pl.semaphore_wait(go_sem, 1)

        own_state(0)

    for k in range(n_tp):
        w_in(2, k).wait()

    with jax.named_scope("fv_next"):
        for t in range(blocks + 2, 2 * blocks + 2):
            if t % per == 0 and 2 + t // per <= len(fv_steps):
                fv_step(2 + t // per)
            gate_slot(t)

    with jax.named_scope("sends"):
        @pl.when(more)
        def _():
            h_out(sp + 1).start()

        own_state(1)

    for i in (3, 4):
        for k in range(n_tp):
            w_in(i, k).wait()

    with jax.named_scope("pool_query"):
        for c in range(chunks - 1):
            weave([(2, project(c, 2, p_buf, BLOCK_ROWS))], [])
        next_state(0, sp == 1)
        weave([(2, project(0, 3, q_buf))], [])
        for c in range(1, chunks):
            weave([(2, project(c, 3, q_buf))], [scores(c - 1), pools(c)])
            if c == 1:
                next_state(1, sp == 1)
        for c in range(1, chunks):
            a_out(0, c).start()

    with jax.named_scope("halo_wait"):
        @pl.when(sp > 0)
        def _():
            h_out(sp).wait_recv()
            p_buf[pl.ds(BLOCK_ROWS - HALO, HALO), :] = halo_in[...]

        next_state(0, sp > 1)

    with jax.named_scope("gate0"):
        weave([(2, project(0, 4, g_buf))], [scores(chunks - 1), pools(0)])
        a_out(0, 0).start()
        next_state(1, sp > 1)

    with jax.named_scope("gate"):
        for c in range(1, chunks):
            weave([(2, project(c, 4, g_buf))], [])

    for i in range(2):
        wo_in(i).wait()
        wo_out(i).wait_recv()
    for c in range(chunks):
        a_out(0, c).wait_recv()
    pool_at, rec_at = (place for _, place in wo_places)

    def out_pool(c):
        rows = rows_of(c)
        for n in range(2):
            cols = slice(n * (feats // 2), (n + 1) * (feats // 2))
            r_buf[rows, cols] = (
                dot(a_own[rows, pool_at], wo_own[pool_at, cols])
                + dot(a_peer[rows, pool_at], wo_peer[pool_at, cols]))
            yield

    with jax.named_scope("out_pool0"):
        weave([(2, out_pool(0))], [])

    def first_state(pr):
        lanes = slice(pr * pair, (pr + 1) * pair)

        @pl.when((sp > 0) & (sp + 1 == n_sp))
        def _():
            st_out(pr).wait_recv()

        @pl.when(sp == 0)
        def _():
            state[:, lanes] = jnp.zeros((DK, pair), F32)

        @pl.when(sp > 0)
        def _():
            state[:, lanes] = state_in[pr].astype(F32)

    with jax.named_scope("join"):
        first_state(0)

    early = blocks // 2
    mix_items = [mix_one(b, h) for pr in range(heads // 2) for b in range(early) for h in (2 * pr, 2 * pr + 1)]
    mix_items += [mix_one(b, h) for b in range(early, blocks) for h in range(heads)]
    per_mix = per * heads

    def mix_slot(t):
        for stage in (3, 2, 1, 0):
            if 0 <= t - stage < len(mix_items):
                next(mix_items[t - stage], None)

    def fold(x):
        acc = x[:, :LANES]
        for k in range(1, x.shape[1] // LANES):
            acc = acc + x[:, k * LANES:(k + 1) * LANES]
        return acc

    first_half = lax.broadcasted_iota(jnp.int32, (32, LANES), 1) < LANES // 2

    def out_one(c, n):
        rows = rows_of(c)
        cols = slice(n * (feats // 2), (n + 1) * (feats // 2))
        full = (dot(a_own[rows, rec_at], wo_own[rec_at, cols])
                + dot(a_peer[rows, rec_at], wo_peer[rec_at, cols]))
        yield
        tile = 32
        for k in range(ROWS // tile):
            part = slice(c * ROWS + k * tile, c * ROWS + (k + 1) * tile)
            here = slice(k * tile, (k + 1) * tile)
            resid = full[here] + (r_buf[part, cols] + ALPHA * x_own[part, cols].astype(F32))
            r_buf[part, cols] = resid
            sums, squares = fold(resid), fold(resid * resid)
            both = jnp.where(first_half, sums + pltpu.roll(sums, LANES // 2, 1),
                             squares + pltpu.roll(squares, LANES // 2, 1))
            stat_own[c, here] = both if n == 0 else stat_own[c, here] + both
        if n == 1:
            s_out(c).start()
        yield

    def norm(c):
        def one(k):
            here = slice(k * 32, (k + 1) * 32)
            both = stat_own[c, here] + stat_peer[c, here]
            mean = jnp.sum(jnp.where(first_half, both, 0.0), axis=1, keepdims=True) / (n_tp * feats)
            square = jnp.sum(jnp.where(first_half, 0.0, both), axis=1, keepdims=True) / (n_tp * feats)
            inv = lax.rsqrt(square - mean * mean + EPS_NORM)
            yield
            part = slice(c * ROWS + k * 32, c * ROWS + (k + 1) * 32)
            for n in range(2):
                cols = slice(n * (feats // 2), (n + 1) * (feats // 2))
                o_buf[part, cols] = (
                    (r_buf[part, cols] - mean) * inv * norm_gain[:, cols] + norm_bias[:, cols]).astype(BF16)
            yield

        for _ in skew([one(k) for k in range(ROWS // 32)], 2, 3)[1]:
            pass
        o_out(c).start()

    with jax.named_scope("out_pool"):
        for c in range(1, chunks):
            weave([(2, out_pool(c))], [(per_mix, (mix_slot((c - 1) * per_mix + t) or t for t in range(per_mix)))])
            if c < heads // 2:
                first_state(c)
        for c in range(early // per):
            a_out(1, c).start()

    out_items = [out_one(c, n) for c in range(chunks) for n in range(2)]

    def out_slot(k):
        for stage in (1, 0):
            if 0 <= k - stage < len(out_items):
                next(out_items[k - stage], None)

    with jax.named_scope("out0"):
        for t in range(3):
            mix_slot((chunks - 1) * per_mix + t)
        for c in range(early // per, chunks - 1):
            a_out(1, c).start()
        a_out(1, 0).wait_recv()
        out_slot(0)
        for t in range(3, 3 + per_mix // 2):
            mix_slot((chunks - 1) * per_mix + t)
        out_slot(1)
        for t in range(3 + per_mix // 2, 3 + per_mix):
            mix_slot((chunks - 1) * per_mix + t)
        a_out(1, chunks - 1).start()

    with jax.named_scope("out1"):
        for c in range(1, chunks - 1):
            a_out(1, c).wait_recv()
        for k in range(2, 2 * chunks - 2):
            out_slot(k)

    with jax.named_scope("out3"):
        a_out(1, chunks - 1).wait_recv()
        for c in range(chunks - 2):
            s_out(c).wait_recv()
        out_slot(2 * chunks - 2)
        for c in range(chunks - 3):
            norm(c)
        out_slot(2 * chunks - 1)
        norm(chunks - 3)
        out_slot(2 * chunks)

    with jax.named_scope("stats"):
        for c in range(chunks - 2, chunks):
            s_out(c).wait_recv()
            norm(c)

    with jax.named_scope("drain"):
        for c in range(chunks):
            x_out(c).wait_send()
            s_out(c).wait_send()
            o_out(c).wait()
            for i in range(2):
                a_out(i, c).wait_send()
        for i in range(2):
            wo_out(i).wait_send()

        @pl.when(more)
        def _():
            for pr in range(heads // 2):
                st_out(pr).wait_send()

        @pl.when(sp + 1 < n_sp)
        def _():
            h_out(sp + 1).wait_send()


def finish(pieces, normed, out, buf, in_sem, out_sem):
    rows = normed.shape[0] // pieces

    def copies(c):
        part = pl.ds(c * rows, rows)
        return (
            pltpu.make_async_copy(normed.at[part], buf.at[part], in_sem.at[c]),
            pltpu.make_async_copy(buf.at[part], out.at[0, part], out_sem.at[c]),
        )

    for c in range(pieces):
        copies(c)[0].start()
    for c in range(pieces):
        copies(c)[0].wait()
        copies(c)[1].start()
    for c in range(pieces):
        copies(c)[1].wait()


def solution(mesh):
    n_sp, n_tp = mesh.shape["sp"], mesh.shape["tp"]

    def local(stream, w_pool, w_query, w_forget, w_value, w_gate, mix, scale, bound, extra,
              gain, wo_pool, wo_rec, norm_gain, norm_bias):
        length, feats = stream.shape[1], stream.shape[2]
        chans, pool_w = bound.shape[0], scale.shape[0]
        blocks = length // BLOCK_ROWS
        chunks = length // ROWS
        pairs = chans // DK // 2
        hbm = pl.BlockSpec(memory_space=pl.ANY)
        dma = pltpu.SemaphoreType.DMA
        scratch = [
            pltpu.VMEM((length, feats), BF16),
            pltpu.VMEM((length, feats), BF16),
            pltpu.VMEM((5, n_tp, feats, chans), BF16),
            pltpu.VMEM((pool_w + chans, feats), BF16),
            pltpu.VMEM((pool_w + chans, feats), BF16),
            pltpu.VMEM((length, pool_w + chans), BF16),
            pltpu.VMEM((length, pool_w + chans), BF16),
            pltpu.VMEM((length, chans), BF16),
            pltpu.VMEM((length, chans), BF16),
            pltpu.VMEM((length, chans), BF16),
            pltpu.VMEM((length, chans), F32),
            pltpu.VMEM((blocks, DK, chans), F32),
            pltpu.VMEM((BLOCK_ROWS + length, pool_w), BF16),
            pltpu.VMEM((length, chans), BF16),
            pltpu.VMEM((length, 2 * chans), BF16),
            pltpu.VMEM((length, chans), BF16),
            pltpu.VMEM((length, max(feats, 2 * chans)), F32),
            pltpu.VMEM((length, feats), BF16),
            pltpu.VMEM((blocks, 8, chans), F32),
            pltpu.VMEM((DK, chans), F32),
            pltpu.VMEM((pairs, DK, 2 * DK), BF16),
            pltpu.VMEM((pairs, DK, 2 * DK), BF16),
            pltpu.VMEM((HALO, pool_w), BF16),
            pltpu.VMEM((chunks, ROWS, LANES), F32),
            pltpu.VMEM((chunks, ROWS, LANES), F32),
            pltpu.VMEM((1, feats), F32),
            pltpu.VMEM((1, feats), F32),
            pltpu.VMEM(mix.shape, BF16),
            pltpu.VMEM((1, pool_w), F32),
            pltpu.VMEM((1, chans), F32),
            pltpu.VMEM((chans // DK, length), F32),
            pltpu.VMEM((length, LANES), F32),
            pltpu.VMEM((1, DK), F32),
            dma((chunks,)), dma((chunks,)), dma((chunks,)), dma((5, n_tp)),
            dma((2,)), dma((2,)), dma((2,)), dma((2, chunks)), dma((2, chunks)),
            dma((pairs,)), dma((pairs,)), dma, dma, dma((chunks,)), dma((chunks,)), dma((chunks,)),
            dma((7,)), pltpu.SemaphoreType.REGULAR, pltpu.SemaphoreType.REGULAR,
        ]
        row = lambda x: x.reshape(1, -1)
        normed = pl.pallas_call(
            functools.partial(mixer, n_sp, n_tp),
            out_shape=jax.ShapeDtypeStruct((length, feats), BF16),
            in_specs=[hbm] * 15,
            out_specs=hbm,
            scratch_shapes=scratch,
            compiler_params=pltpu.CompilerParams(
                collective_id=0, has_side_effects=True, vmem_limit_bytes=60 * 1024 * 1024),
            name="mixer",
        )(stream, w_pool, w_query, w_forget, w_value, w_gate, mix, row(scale), row(bound), extra.T,
          row(gain), wo_pool, wo_rec, row(norm_gain), row(norm_bias))
        pieces = 8
        return pl.pallas_call(
            functools.partial(finish, pieces),
            out_shape=jax.ShapeDtypeStruct(stream.shape, BF16),
            in_specs=[hbm],
            out_specs=hbm,
            scratch_shapes=[pltpu.VMEM((length, feats), BF16), dma((pieces,)), dma((pieces,))],
            compiler_params=pltpu.CompilerParams(vmem_limit_bytes=60 * 1024 * 1024),
            name="finish",
        )(normed)

    placed = (
        P("fs", "sp", "tp"), P(None, "tp"), P(None, "tp"), P(None, "tp"), P(None, "tp"),
        P(None, "tp"), P("tp", None, None), P("tp"), P("tp"), P("sp", "tp"), P(),
        P("tp", None), P("tp", None), P("tp"), P("tp"),
    )
    return jax.shard_map(
        local, mesh=mesh, in_specs=placed, out_specs=P("fs", "sp", "tp"), check_vma=False
    )
```

```python
import functools

import jax
import jax.numpy as jnp
from jax import lax
from jax.experimental import pallas as pl
from jax.experimental.pallas import tpu as pltpu
from jax.sharding import PartitionSpec as P

DK = 128
BLOCK_ROWS = 128
GROUP_CH = 256
HALO = 16
LANES = 128
ROWS = 256

ALPHA = 2.0**0.25
EPS_RMS = 1e-06
EPS_NORM = 1e-05
F32 = jnp.float32
BF16 = jnp.bfloat16
NT = (((1,), (1,)), ((), ()))
TN = (((0,), (0,)), ((), ()))
MESH = pl.DeviceIdType.MESH


def dot(a, b, dims=None):
    if dims is None:
        return jnp.dot(a, b, preferred_element_type=F32)
    return lax.dot_general(a, b, dims, preferred_element_type=F32)


def half_sigmoid(x):
    return 0.5 + 0.5 * jnp.tanh(0.5 * x)


def skew(items, stages, lag=1):
    items, count = list(items), 0
    order = []
    for t in range(len(items) + lag * (stages - 1)):
        for stage in reversed(range(stages)):
            if 0 <= t - stage * lag < len(items):
                order.append(t - stage * lag)
                count += 1

    def run():
        for i in order:
            next(items[i], None)
            yield

    return count, run()


def weave(bigs, smalls):
    n_big, n_small = (sum(n for n, _ in steps) for steps in (bigs, smalls))
    rest = [step for _, steps in smalls for step in [steps]]
    small = (None for steps in rest for _ in steps)
    done = 0
    for i, _ in enumerate(piece for _, steps in bigs for piece in steps):
        want = -(-(i + 1) * n_small // n_big)
        while done < want:
            next(small, None)
            done += 1
    for _ in small:
        pass


def mixer(
    n_sp, n_tp,
    stream, w_pool, w_query, w_forget, w_value, w_gate,
    mix_in, scale_in, bound_in, extra_in, gain_in, wo_pool, wo_rec, norm_gain_in, norm_bias_in,
    out,
    x_own, x_peer, w_buf, fv_buf, wo_own, wo_peer, a_own, a_peer, f_buf, v_buf, u_buf, e_buf, t_buf, p_buf, q_buf, sq_buf, g_buf, r_buf,
    o_buf, half_buf, state, state_out, state_in, halo_in, stat_own, stat_peer, norm_gain, norm_bias,
    mix, scale, bound, extra, extra_t, gain,
    x_loc, x_send, x_recv, w_sem, fv_sem, wo_loc, wo_send, wo_recv, a_send, a_recv,
    st_send, st_recv, h_send, h_recv, s_send, s_recv, o_sem, small_sem, met_sem, go_sem,
):
    sp, tp = lax.axis_index("sp"), lax.axis_index("tp")
    peer = 1 - tp
    length, feats = stream.shape[1], stream.shape[2]
    chans = bound.shape[1]
    heads = chans // DK
    pool_w = scale.shape[1]
    groups = mix.shape[0]
    chunks = length // ROWS
    blocks = length // BLOCK_ROWS
    per = ROWS // BLOCK_ROWS
    pair = 2 * DK

    def rows_of(c, size=ROWS, base=0):
        start = c * size + base
        return pl.ds(start if isinstance(start, int) else pl.multiple_of(start, BLOCK_ROWS), size)

    def x_in(c):
        rows = rows_of(c)
        return pltpu.make_async_copy(stream.at[0, rows], x_own.at[rows], x_loc.at[c])

    def x_out(c):
        rows = rows_of(c)
        return pltpu.make_async_remote_copy(
            x_own.at[rows], x_peer.at[rows], x_send.at[c], x_recv.at[c],
            device_id={"tp": peer}, device_id_type=MESH)

    def w_rows(k):
        return pl.ds(pl.multiple_of((tp, peer)[k] * feats, LANES), feats)

    def w_in(i, k):
        src = (w_pool, w_query, w_gate)[i]
        return pltpu.make_async_copy(src.at[w_rows(k)], w_buf.at[i, k], w_sem.at[i, k])

    def fv_in(pr, k):
        return [
            pltpu.make_async_copy(
                src.at[w_rows(k), pl.ds(pr * pair, pair)], fv_buf.at[pr, k, :, pl.ds(i * pair, pair)],
                fv_sem.at[pr, k, i])
            for i, src in enumerate((w_forget, w_value))]

    my_cols = pl.ds(pl.multiple_of(tp * feats, LANES), feats)
    peer_cols = pl.ds(pl.multiple_of(peer * feats, LANES), feats)
    wo_places = ((wo_pool, pl.ds(0, pool_w)), (wo_rec, pl.ds(pool_w, chans)))

    def wo_in(i):
        src, place = wo_places[i]
        return pltpu.make_async_copy(src.at[:, my_cols], wo_own.at[place], wo_loc.at[i])

    def wo_out(i):
        src, place = wo_places[i]
        return pltpu.make_async_remote_copy(
            src.at[:, peer_cols], wo_peer.at[place], wo_send.at[i], wo_recv.at[i],
            device_id={"tp": peer}, device_id_type=MESH)

    def a_out(i, c):
        rows, cols = rows_of(c), wo_places[i][1]
        return pltpu.make_async_remote_copy(
            a_own.at[rows, cols], a_peer.at[rows, cols], a_send.at[i, c], a_recv.at[i, c],
            device_id={"tp": peer}, device_id_type=MESH)

    def st_out(pr):
        return pltpu.make_async_remote_copy(
            state_out.at[pr], state_in.at[pr], st_send.at[pr], st_recv.at[pr],
            device_id={"sp": lax.rem(sp + 1, n_sp)}, device_id_type=MESH)

    def h_out(k):
        return pltpu.make_async_remote_copy(
            p_buf.at[pl.ds(BLOCK_ROWS + length - HALO, HALO)], halo_in, h_send, h_recv,
            device_id={"sp": k}, device_id_type=MESH)

    def s_out(c):
        return pltpu.make_async_remote_copy(
            stat_own.at[c], stat_peer.at[c], s_send.at[c], s_recv.at[c],
            device_id={"tp": peer}, device_id_type=MESH)

    def o_out(c):
        rows = rows_of(c)
        return pltpu.make_async_copy(o_buf.at[rows], out.at[rows], o_sem.at[c])

    smalls = [
        pltpu.make_async_copy(src, dst, small_sem.at[i])
        for i, (src, dst) in enumerate(
            ((bound_in, bound), (extra_in, extra), (mix_in, mix), (scale_in, scale), (gain_in, gain),
             (norm_gain_in, norm_gain), (norm_bias_in, norm_bias)))
    ]

    barrier = pltpu.get_barrier_semaphore()

    @pl.when(tp == 0)
    def _():
        pl.semaphore_signal(barrier, inc=1, device_id={"tp": peer}, device_id_type=MESH)

    n_pairs = heads // 2
    x_in(0).start()
    for copy in fv_in(0, 0):
        copy.start()
    @pl.when(tp > 0)
    def _():
        pl.semaphore_wait(barrier, 1)
        pl.semaphore_signal(met_sem, inc=1, device_id={"tp": peer}, device_id_type=MESH)

    @pl.when(tp == 0)
    def _():
        pl.semaphore_wait(met_sem, 1)

    @pl.when((tp == 0) & (sp > 0))
    def _():
        pl.semaphore_signal(barrier, inc=1, device_id={"sp": lax.rem(sp + n_sp - 1, n_sp)}, device_id_type=MESH)

    for c in range(1, chunks):
        x_in(c).start()
    for pr in range(1, n_pairs):
        for copy in fv_in(pr, 0):
            copy.start()
    for copy in smalls:
        copy.start()

    p_buf[pl.ds(0, BLOCK_ROWS), :] = jnp.zeros((BLOCK_ROWS, pool_w), BF16)
    state[...] = jnp.zeros_like(state)

    row_ids = lax.broadcasted_iota(jnp.int32, (BLOCK_ROWS, BLOCK_ROWS), 0)
    col_ids = lax.broadcasted_iota(jnp.int32, (BLOCK_ROWS, BLOCK_ROWS), 1)
    lower = row_ids >= col_ids
    tri = jnp.where(lower, 1.0, 0.0).astype(BF16)
    tri_twice = jnp.concatenate([tri, tri], axis=1)

    def own_fv(c, pr):
        rows = rows_of(c)
        r_buf[rows, 2 * pr * pair:2 * (pr + 1) * pair] = dot(x_own[rows], fv_buf[pr, 0])

    def peer_fv(c, pr):
        rows = rows_of(c)
        cols = slice(pr * pair, (pr + 1) * pair)
        part = dot(x_peer[rows], fv_buf[pr, 1])
        for i, buf in ((0, f_buf), (1, v_buf)):
            base = (2 * pr + i) * pair
            buf[rows, cols] = (r_buf[rows, base:base + pair] + part[:, i * pair:(i + 1) * pair]).astype(BF16)
        yield

    def project(c, i, buf, base=0):
        rows = rows_of(c)
        part = dot(x_own[rows], w_buf[i, 0])
        yield
        buf[rows_of(c, ROWS, base), :] = (part + dot(x_peer[rows], w_buf[i, 1])).astype(BF16)
        yield

    def gate_one(b, pr):
        brows = rows_of(b, BLOCK_ROWS)
        lanes = slice(pr * pair, (pr + 1) * pair)
        tile = BLOCK_ROWS // 4
        tiles = [slice(b * BLOCK_ROWS + k * tile, b * BLOCK_ROWS + (k + 1) * tile) for k in range(4)]
        weights, highs, lows = [], [], []
        for part in tiles:
            f_in = f_buf[part, lanes].astype(F32)
            drop = jnp.concatenate(
                [jnp.broadcast_to(extra_t[part, h:h + 1], (tile, DK)) for h in (2 * pr, 2 * pr + 1)], axis=1)
            weight = (1.0 - bound[:, lanes]) * (0.5 - 0.5 * jnp.tanh(0.5 * f_in))
            keep = jnp.log(1.0 - weight) + drop
            high = keep.astype(BF16)
            highs.append(high)
            lows.append((keep - high.astype(F32)).astype(BF16))
            e_buf[part, lanes] = weight
        total = dot(tri_twice, jnp.concatenate(highs + lows, axis=0))
        yield
        middle = 0.5 * total[BLOCK_ROWS - 1:BLOCK_ROWS]
        half = jnp.exp(middle)
        half_buf[b, :, lanes] = jnp.broadcast_to(half, (8, pair))
        downs = []
        for k, part in enumerate(tiles):
            apart = total[k * tile:(k + 1) * tile] - middle
            down = (e_buf[part, lanes] * jnp.exp(-apart)).astype(BF16)
            downs.append(down)
            u_buf[part, lanes] = down
            e_buf[part, lanes] = jnp.exp(apart)
        down = jnp.concatenate(downs, axis=0)
        terms = [
            dot(v_buf[brows, pr * pair + j * DK:pr * pair + (j + 1) * DK], down[:, j * DK:(j + 1) * DK], TN)
            for j in range(2)]
        yield
        term = jnp.concatenate(terms, axis=1) * half
        t_buf[b, :, lanes] = term
        state[:, lanes] = half * half * state[:, lanes] + term
        yield

    def gates(c, pr):
        return skew([gate_one(c * per + k, pr) for k in range(per)], 3)

    back = (lax.broadcasted_iota(jnp.int32, (BLOCK_ROWS, 2 * BLOCK_ROWS), 0) + BLOCK_ROWS
            - lax.broadcasted_iota(jnp.int32, (BLOCK_ROWS, 2 * BLOCK_ROWS), 1))
    count = lax.broadcasted_iota(jnp.int32, (BLOCK_ROWS, LANES), 0) + (sp * length + 1)

    def pool_one(b, j):
        start = b * BLOCK_ROWS
        brows = rows_of(b, BLOCK_ROWS)
        lanes = slice(j * GROUP_CH, (j + 1) * GROUP_CH)
        near = p_buf[rows_of(b, BLOCK_ROWS, 0), lanes]
        here = p_buf[rows_of(b, BLOCK_ROWS, BLOCK_ROWS), lanes]
        window = jnp.left_shift(jnp.int32(2), tp * groups + j)
        band = jnp.where((back >= 0) & (back < window), 1.0, 0.0).astype(BF16)
        sums = dot(band, jnp.concatenate([near, here], axis=0))
        yield
        share = 1.0 / jnp.minimum(count + start, window).astype(F32)
        share = jnp.concatenate([share] * (GROUP_CH // LANES), axis=1)
        diff = (sums * share - here.astype(F32)).astype(BF16)
        mixed = dot(diff, mix[j])
        yield
        a_own[brows, lanes] = (mixed * scale[:, lanes]).astype(BF16)
        yield

    def pools(c):
        return skew([pool_one(c * per + k, j) for k in range(per) for j in range(groups)], 3)

    def score_one(b, h):
        brows = rows_of(b, BLOCK_ROWS)
        lanes = slice(h * DK, (h + 1) * DK)
        q_in = q_buf[brows, lanes].astype(F32)
        up = (q_in * half_sigmoid(q_in) * e_buf[brows, lanes]).astype(BF16)
        sq_buf[brows, h * pair + DK:(h + 1) * pair] = up
        tile = dot(up, u_buf[brows, lanes], NT)
        yield
        sq_buf[brows, h * pair:h * pair + DK] = jnp.where(lower, tile, 0.0).astype(BF16)
        yield

    def scores(c):
        return skew([score_one(c * per + k, h) for k in range(per) for h in range(heads)], 2, 2)

    def mix_one(b, h):
        brows = rows_of(b, BLOCK_ROWS)
        lanes = slice(h * DK, (h + 1) * DK)
        half = half_buf[b, 0:1, lanes]
        before = state[:, lanes] * half
        state[:, lanes] = before * half + t_buf[b, :, lanes]
        carried = jnp.transpose(before.astype(BF16))
        yield
        raw = dot(sq_buf[brows, h * pair:(h + 1) * pair],
                  jnp.concatenate([v_buf[brows, lanes], carried], axis=0))
        yield
        power = jnp.mean(raw * raw, axis=-1, keepdims=True)
        yield
        gate = g_buf[brows, lanes].astype(F32)
        rec = raw * lax.rsqrt(power + EPS_RMS) * gain[...] * (gate * half_sigmoid(gate))
        a_own[brows, pool_w + h * DK:pool_w + (h + 1) * DK] = rec.astype(BF16)
        yield

    def mixes(c):
        return skew([mix_one(c * per + k, h) for k in range(per) for h in range(heads)], 4)

    with jax.named_scope("own_fv"):
        x_in(0).wait()
        x_out(0).start()
        for copy in fv_in(0, 0):
            copy.wait()
        own_fv(0, 0)
        for c in range(1, chunks):
            x_in(c).wait()
            x_out(c).start()
        for pr in range(n_pairs):
            for copy in fv_in(pr, 1):
                copy.start()
        for c in range(1, chunks):
            own_fv(c, 0)
        for pr in range(1, n_pairs):
            for copy in fv_in(pr, 0):
                copy.wait()
        for copy in smalls:
            copy.wait()
        for b in range(blocks):
            brows = rows_of(b, BLOCK_ROWS)
            extra_t[brows, 0:heads] = jnp.transpose(extra[:, brows])
        for pr in range(1, n_pairs):
            for c in range(chunks):
                own_fv(c, pr)

    for i in range(3):
        for k in range(n_tp):
            w_in(i, k).start()
    for i in range(2):
        wo_in(i).start()
        wo_out(i).start()

    more = sp + 1 < n_sp

    def own_state(pr):
        @pl.when((sp == 0) & more)
        def _():
            state_out[pr] = state[:, pr * pair:(pr + 1) * pair].astype(BF16)
            st_out(pr).start()

    def next_state(pr, here):
        @pl.when(here & (sp > 0) & more)
        def _():
            lanes = slice(pr * pair, (pr + 1) * pair)
            root = half_buf[0, 0:1, lanes]
            for b in range(1, blocks):
                root = root * half_buf[b, 0:1, lanes]
            st_out(pr).wait_recv()
            state_out[pr] = (root * root * state_in[pr].astype(F32) + state[:, lanes]).astype(BF16)
            st_out(pr).start()

    fv_steps = [(c, pr) for pr in range(heads // 2) for c in range(chunks)]
    gate_items = [gate_one(b, pr) for pr in range(heads // 2) for b in range(blocks)]

    def fv_step(k):
        if k >= len(fv_steps):
            for _ in project(chunks - 1, 0, p_buf, BLOCK_ROWS):
                pass
            return
        c, pr = fv_steps[k]
        if pr == 0 and c % 2 == 0:
            for d in (c, c + 1):
                x_out(d).wait_recv()
        for _ in peer_fv(c, pr):
            pass

    def gate_slot(t):
        for stage in (2, 1, 0):
            if 0 <= t - stage < len(gate_items):
                next(gate_items[t - stage], None)

    for pr in range(n_pairs):
        for copy in fv_in(pr, 1):
            copy.wait()
    with jax.named_scope("fv"):
        fv_step(0)
        fv_step(1)
        for t in range(blocks + 2):
            if t % per == 0:
                fv_step(2 + t // per)
            gate_slot(t)

    with jax.named_scope("greet_wait"):
        @pl.when((tp == 0) & more)
        def _():
            pl.semaphore_wait(barrier, 1)
            pl.semaphore_signal(go_sem, inc=1, device_id={"tp": peer}, device_id_type=MESH)

        @pl.when((tp > 0) & more)
        def _():
            pl.semaphore_wait(go_sem, 1)

        own_state(0)

    for k in range(n_tp):
        w_in(0, k).wait()

    with jax.named_scope("fv_next"):
        for t in range(blocks + 2, 2 * blocks + 2):
            if t % per == 0 and 2 + t // per <= len(fv_steps):
                fv_step(2 + t // per)
            gate_slot(t)

    with jax.named_scope("sends"):
        @pl.when(more)
        def _():
            h_out(sp + 1).start()

        own_state(1)

    for i in (1, 2):
        for k in range(n_tp):
            w_in(i, k).wait()

    with jax.named_scope("pool_query"):
        for c in range(chunks - 1):
            weave([(2, project(c, 0, p_buf, BLOCK_ROWS))], [])
        next_state(0, sp == 1)
        weave([(2, project(0, 1, q_buf))], [])
        for c in range(1, chunks):
            weave([(2, project(c, 1, q_buf))], [scores(c - 1), pools(c)])
            if c == 1:
                next_state(1, sp == 1)
        for c in range(1, chunks):
            a_out(0, c).start()

    with jax.named_scope("halo_wait"):
        @pl.when(sp > 0)
        def _():
            h_out(sp).wait_recv()
            p_buf[pl.ds(BLOCK_ROWS - HALO, HALO), :] = halo_in[...]

        next_state(0, sp > 1)

    with jax.named_scope("gate0"):
        weave([(2, project(0, 2, g_buf))], [scores(chunks - 1), pools(0)])
        a_out(0, 0).start()
        next_state(1, sp > 1)

    with jax.named_scope("gate"):
        for c in range(1, chunks):
            weave([(2, project(c, 2, g_buf))], [])

    for i in range(2):
        wo_in(i).wait()
        wo_out(i).wait_recv()
    for c in range(chunks):
        a_out(0, c).wait_recv()
    pool_at, rec_at = (place for _, place in wo_places)

    def out_pool(c):
        rows = rows_of(c)
        for n in range(2):
            cols = slice(n * (feats // 2), (n + 1) * (feats // 2))
            r_buf[rows, cols] = (
                dot(a_own[rows, pool_at], wo_own[pool_at, cols])
                + dot(a_peer[rows, pool_at], wo_peer[pool_at, cols]))
            yield

    with jax.named_scope("out_pool0"):
        weave([(2, out_pool(0))], [])

    def first_state(pr):
        lanes = slice(pr * pair, (pr + 1) * pair)

        @pl.when((sp > 0) & (sp + 1 == n_sp))
        def _():
            st_out(pr).wait_recv()

        @pl.when(sp == 0)
        def _():
            state[:, lanes] = jnp.zeros((DK, pair), F32)

        @pl.when(sp > 0)
        def _():
            state[:, lanes] = state_in[pr].astype(F32)

    with jax.named_scope("join"):
        first_state(0)

    mix_items = [
        mix_one(c * per + k, h) for c in range(chunks) for pr in range(n_pairs) for k in range(per)
        for h in (2 * pr, 2 * pr + 1)]
    per_mix = per * heads

    def mix_slot(t):
        for stage in (3, 2, 1, 0):
            if 0 <= t - stage < len(mix_items):
                next(mix_items[t - stage], None)

    def fold(x):
        acc = x[:, :LANES]
        for k in range(1, x.shape[1] // LANES):
            acc = acc + x[:, k * LANES:(k + 1) * LANES]
        return acc

    first_half = lax.broadcasted_iota(jnp.int32, (32, LANES), 1) < LANES // 2

    def out_one(c, n):
        rows = rows_of(c)
        cols = slice(n * (feats // 2), (n + 1) * (feats // 2))
        full = (dot(a_own[rows, rec_at], wo_own[rec_at, cols])
                + dot(a_peer[rows, rec_at], wo_peer[rec_at, cols]))
        yield
        tile = 32
        for k in range(ROWS // tile):
            part = slice(c * ROWS + k * tile, c * ROWS + (k + 1) * tile)
            here = slice(k * tile, (k + 1) * tile)
            resid = full[here] + (r_buf[part, cols] + ALPHA * x_own[part, cols].astype(F32))
            r_buf[part, cols] = resid
            sums, squares = fold(resid), fold(resid * resid)
            both = jnp.where(first_half, sums + pltpu.roll(sums, LANES // 2, 1),
                             squares + pltpu.roll(squares, LANES // 2, 1))
            stat_own[c, here] = both if n == 0 else stat_own[c, here] + both
        if n == 1:
            s_out(c).start()
        yield

    def norm(c):
        def one(k):
            here = slice(k * 32, (k + 1) * 32)
            both = stat_own[c, here] + stat_peer[c, here]
            mean = jnp.sum(jnp.where(first_half, both, 0.0), axis=1, keepdims=True) / (n_tp * feats)
            square = jnp.sum(jnp.where(first_half, 0.0, both), axis=1, keepdims=True) / (n_tp * feats)
            inv = lax.rsqrt(square - mean * mean + EPS_NORM)
            yield
            part = slice(c * ROWS + k * 32, c * ROWS + (k + 1) * 32)
            for n in range(2):
                cols = slice(n * (feats // 2), (n + 1) * (feats // 2))
                o_buf[part, cols] = (
                    (r_buf[part, cols] - mean) * inv * norm_gain[:, cols] + norm_bias[:, cols]).astype(BF16)
            yield

        for _ in skew([one(k) for k in range(ROWS // 32)], 2, 3)[1]:
            pass
        o_out(c).start()

    def mix_slots(first, last):
        for t in range(first, min(last, len(mix_items) + 3)):
            mix_slot(t)
            if t % per_mix == 2 and t >= per_mix:
                a_out(1, t // per_mix - 1).start()

    pieces = [(c, n) for c in range(1, chunks) for n in range(2)]
    per_piece = -(-(len(mix_items) + 3) // (len(pieces) + 1))

    with jax.named_scope("out_pool"):
        for k, (c, n) in enumerate(pieces):
            if n == 0:
                step = out_pool(c)
            next(step, None)
            if k == 0:
                mix_slots(0, per_mix // n_pairs)
                for pr in range(1, n_pairs):
                    first_state(pr)
                mix_slots(per_mix // n_pairs, per_piece)
            else:
                mix_slots(k * per_piece, (k + 1) * per_piece)

    out_items = [out_one(c, n) for c in range(chunks) for n in range(2)]

    def out_slot(k):
        for stage in (0, 1):
            if 0 <= k - stage < len(out_items):
                next(out_items[k - stage], None)

    with jax.named_scope("out0"):
        a_out(1, 0).wait_recv()
        out_slot(0)
        mix_slots(len(pieces) * per_piece, len(mix_items) + 3)
        out_slot(1)

    with jax.named_scope("out2"):
        for c in range(1, chunks - 1):
            a_out(1, c).wait_recv()
        for k in range(2, 2 * chunks - 2):
            out_slot(k)

    with jax.named_scope("out3"):
        a_out(1, chunks - 1).wait_recv()
        out_slot(2 * chunks - 2)
        out_slot(2 * chunks - 1)
        for c in range(chunks - 3):
            s_out(c).wait_recv()
            norm(c)
        out_slot(2 * chunks)

    with jax.named_scope("stats"):
        for c in range(chunks - 3, chunks):
            s_out(c).wait_recv()
            norm(c)

    with jax.named_scope("drain"):
        for c in range(chunks):
            x_out(c).wait_send()
            s_out(c).wait_send()
            o_out(c).wait()
            for i in range(2):
                a_out(i, c).wait_send()
        for i in range(2):
            wo_out(i).wait_send()

        @pl.when(more)
        def _():
            for pr in range(heads // 2):
                st_out(pr).wait_send()

        @pl.when(sp + 1 < n_sp)
        def _():
            h_out(sp + 1).wait_send()


def finish(pieces, normed, out, buf, in_sem, out_sem):
    rows = normed.shape[0] // pieces

    def copies(c):
        part = pl.ds(c * rows, rows)
        return (
            pltpu.make_async_copy(normed.at[part], buf.at[part], in_sem.at[c]),
            pltpu.make_async_copy(buf.at[part], out.at[0, part], out_sem.at[c]),
        )

    for c in range(pieces):
        copies(c)[0].start()
    for c in range(pieces):
        copies(c)[0].wait()
        copies(c)[1].start()
    for c in range(pieces):
        copies(c)[1].wait()


def solution(mesh):
    n_sp, n_tp = mesh.shape["sp"], mesh.shape["tp"]

    def local(stream, w_pool, w_query, w_forget, w_value, w_gate, mix, scale, bound, extra,
              gain, wo_pool, wo_rec, norm_gain, norm_bias):
        length, feats = stream.shape[1], stream.shape[2]
        chans, pool_w = bound.shape[0], scale.shape[0]
        blocks = length // BLOCK_ROWS
        chunks = length // ROWS
        pairs = chans // DK // 2
        hbm = pl.BlockSpec(memory_space=pl.ANY)
        dma = pltpu.SemaphoreType.DMA
        scratch = [
            pltpu.VMEM((length, feats), BF16),
            pltpu.VMEM((length, feats), BF16),
            pltpu.VMEM((3, n_tp, feats, chans), BF16),
            pltpu.VMEM((pairs, n_tp, feats, 4 * DK), BF16),
            pltpu.VMEM((pool_w + chans, feats), BF16),
            pltpu.VMEM((pool_w + chans, feats), BF16),
            pltpu.VMEM((length, pool_w + chans), BF16),
            pltpu.VMEM((length, pool_w + chans), BF16),
            pltpu.VMEM((length, chans), BF16),
            pltpu.VMEM((length, chans), BF16),
            pltpu.VMEM((length, chans), BF16),
            pltpu.VMEM((length, chans), F32),
            pltpu.VMEM((blocks, DK, chans), F32),
            pltpu.VMEM((BLOCK_ROWS + length, pool_w), BF16),
            pltpu.VMEM((length, chans), BF16),
            pltpu.VMEM((length, 2 * chans), BF16),
            pltpu.VMEM((length, chans), BF16),
            pltpu.VMEM((length, max(feats, 2 * chans)), F32),
            pltpu.VMEM((length, feats), BF16),
            pltpu.VMEM((blocks, 8, chans), F32),
            pltpu.VMEM((DK, chans), F32),
            pltpu.VMEM((pairs, DK, 2 * DK), BF16),
            pltpu.VMEM((pairs, DK, 2 * DK), BF16),
            pltpu.VMEM((HALO, pool_w), BF16),
            pltpu.VMEM((chunks, ROWS, LANES), F32),
            pltpu.VMEM((chunks, ROWS, LANES), F32),
            pltpu.VMEM((1, feats), F32),
            pltpu.VMEM((1, feats), F32),
            pltpu.VMEM(mix.shape, BF16),
            pltpu.VMEM((1, pool_w), F32),
            pltpu.VMEM((1, chans), F32),
            pltpu.VMEM((chans // DK, length), F32),
            pltpu.VMEM((length, LANES), F32),
            pltpu.VMEM((1, DK), F32),
            dma((chunks,)), dma((chunks,)), dma((chunks,)), dma((3, n_tp)), dma((pairs, n_tp, 2)),
            dma((2,)), dma((2,)), dma((2,)), dma((2, chunks)), dma((2, chunks)),
            dma((pairs,)), dma((pairs,)), dma, dma, dma((chunks,)), dma((chunks,)), dma((chunks,)),
            dma((7,)), pltpu.SemaphoreType.REGULAR, pltpu.SemaphoreType.REGULAR,
        ]
        row = lambda x: x.reshape(1, -1)
        normed = pl.pallas_call(
            functools.partial(mixer, n_sp, n_tp),
            out_shape=jax.ShapeDtypeStruct((length, feats), BF16),
            in_specs=[hbm] * 15,
            out_specs=hbm,
            scratch_shapes=scratch,
            compiler_params=pltpu.CompilerParams(
                collective_id=0, has_side_effects=True, vmem_limit_bytes=60 * 1024 * 1024),
            name="mixer",
        )(stream, w_pool, w_query, w_forget, w_value, w_gate, mix, row(scale), row(bound), extra.T,
          row(gain), wo_pool, wo_rec, row(norm_gain), row(norm_bias))
        pieces = 4
        return pl.pallas_call(
            functools.partial(finish, pieces),
            out_shape=jax.ShapeDtypeStruct(stream.shape, BF16),
            in_specs=[hbm],
            out_specs=hbm,
            scratch_shapes=[pltpu.VMEM((length, feats), BF16), dma((pieces,)), dma((pieces,))],
            compiler_params=pltpu.CompilerParams(vmem_limit_bytes=60 * 1024 * 1024),
            name="finish",
        )(normed)

    placed = (
        P("fs", "sp", "tp"), P(None, "tp"), P(None, "tp"), P(None, "tp"), P(None, "tp"),
        P(None, "tp"), P("tp", None, None), P("tp"), P("tp"), P("sp", "tp"), P(),
        P("tp", None), P("tp", None), P("tp"), P("tp"),
    )
    return jax.shard_map(
        local, mesh=mesh, in_specs=placed, out_specs=P("fs", "sp", "tp"), check_vma=False
    )
```

```python
import functools

import jax
import jax.numpy as jnp
from jax import lax
from jax.experimental import pallas as pl
from jax.experimental.pallas import tpu as pltpu
from jax.sharding import PartitionSpec as P

DK = 128
BLOCK_ROWS = 128
GROUP_CH = 256
HALO = 16
LANES = 128
ROWS = 256

ALPHA = 2.0**0.25
EPS_RMS = 1e-06
EPS_NORM = 1e-05
F32 = jnp.float32
BF16 = jnp.bfloat16
NT = (((1,), (1,)), ((), ()))
TN = (((0,), (0,)), ((), ()))
MESH = pl.DeviceIdType.MESH


def dot(a, b, dims=None):
    if dims is None:
        return jnp.dot(a, b, preferred_element_type=F32)
    return lax.dot_general(a, b, dims, preferred_element_type=F32)


def half_sigmoid(x):
    return 0.5 + 0.5 * jnp.tanh(0.5 * x)


def skew(items, stages, lag=1):
    items, count = list(items), 0
    order = []
    for t in range(len(items) + lag * (stages - 1)):
        for stage in reversed(range(stages)):
            if 0 <= t - stage * lag < len(items):
                order.append(t - stage * lag)
                count += 1

    def run():
        for i in order:
            next(items[i], None)
            yield

    return count, run()


def weave(bigs, smalls):
    n_big, n_small = (sum(n for n, _ in steps) for steps in (bigs, smalls))
    rest = [step for _, steps in smalls for step in [steps]]
    small = (None for steps in rest for _ in steps)
    done = 0
    for i, _ in enumerate(piece for _, steps in bigs for piece in steps):
        want = -(-(i + 1) * n_small // n_big)
        while done < want:
            next(small, None)
            done += 1
    for _ in small:
        pass


def mixer(
    n_sp, n_tp,
    stream, w_pool, w_query, w_forget, w_value, w_gate,
    mix_in, scale_in, bound_in, extra_in, gain_in, wo_pool, wo_rec, norm_gain_in, norm_bias_in,
    out,
    x_own, x_peer, w_buf, fv_buf, wo_own, wo_peer, a_own, a_peer, f_buf, v_buf, u_buf, e_buf, t_buf, p_buf, q_buf, sq_buf, g_buf, r_buf,
    o_buf, half_buf, state, state_out, state_in, halo_in, stat_own, stat_peer, norm_gain, norm_bias,
    mix, scale, bound, extra, extra_t, gain,
    x_loc, x_send, x_recv, w_sem, fv_sem, wo_loc, wo_send, wo_recv, a_send, a_recv,
    st_send, st_recv, h_send, h_recv, s_send, s_recv, o_sem, small_sem, met_sem, go_sem,
):
    sp, tp = lax.axis_index("sp"), lax.axis_index("tp")
    peer = 1 - tp
    length, feats = stream.shape[1], stream.shape[2]
    chans = bound.shape[1]
    heads = chans // DK
    pool_w = scale.shape[1]
    groups = mix.shape[0]
    chunks = length // ROWS
    blocks = length // BLOCK_ROWS
    per = ROWS // BLOCK_ROWS
    pair = 2 * DK

    def rows_of(c, size=ROWS, base=0):
        start = c * size + base
        return pl.ds(start if isinstance(start, int) else pl.multiple_of(start, BLOCK_ROWS), size)

    def x_in(c):
        rows = rows_of(c)
        return pltpu.make_async_copy(stream.at[0, rows], x_own.at[rows], x_loc.at[c])

    def x_out(c):
        rows = rows_of(c)
        return pltpu.make_async_remote_copy(
            x_own.at[rows], x_peer.at[rows], x_send.at[c], x_recv.at[c],
            device_id={"tp": peer}, device_id_type=MESH)

    def w_rows(k):
        return pl.ds(pl.multiple_of((tp, peer)[k] * feats, LANES), feats)

    def w_in(i, k):
        src = (w_pool, w_query, w_gate)[i]
        return pltpu.make_async_copy(src.at[w_rows(k)], w_buf.at[i, k], w_sem.at[i, k])

    def fv_in(pr, k):
        return [
            pltpu.make_async_copy(
                src.at[w_rows(k), pl.ds(pr * pair, pair)], fv_buf.at[pr, k, :, pl.ds(i * pair, pair)],
                fv_sem.at[pr, k, i])
            for i, src in enumerate((w_forget, w_value))]

    my_cols = pl.ds(pl.multiple_of(tp * feats, LANES), feats)
    peer_cols = pl.ds(pl.multiple_of(peer * feats, LANES), feats)
    wo_places = ((wo_pool, pl.ds(0, pool_w)), (wo_rec, pl.ds(pool_w, chans)))

    def wo_in(i):
        src, place = wo_places[i]
        return pltpu.make_async_copy(src.at[:, my_cols], wo_own.at[place], wo_loc.at[i])

    def wo_out(i):
        src, place = wo_places[i]
        return pltpu.make_async_remote_copy(
            src.at[:, peer_cols], wo_peer.at[place], wo_send.at[i], wo_recv.at[i],
            device_id={"tp": peer}, device_id_type=MESH)

    def a_out(i, c):
        rows, cols = rows_of(c), wo_places[i][1]
        return pltpu.make_async_remote_copy(
            a_own.at[rows, cols], a_peer.at[rows, cols], a_send.at[i, c], a_recv.at[i, c],
            device_id={"tp": peer}, device_id_type=MESH)

    def st_out(pr):
        return pltpu.make_async_remote_copy(
            state_out.at[pr], state_in.at[pr], st_send.at[pr], st_recv.at[pr],
            device_id={"sp": lax.rem(sp + 1, n_sp)}, device_id_type=MESH)

    def h_out(k):
        return pltpu.make_async_remote_copy(
            p_buf.at[pl.ds(BLOCK_ROWS + length - HALO, HALO)], halo_in, h_send, h_recv,
            device_id={"sp": k}, device_id_type=MESH)

    def s_out(c):
        return pltpu.make_async_remote_copy(
            stat_own.at[c], stat_peer.at[c], s_send.at[c], s_recv.at[c],
            device_id={"tp": peer}, device_id_type=MESH)

    def o_out(c):
        rows = rows_of(c)
        return pltpu.make_async_copy(o_buf.at[rows], out.at[rows], o_sem.at[c])

    smalls = [
        pltpu.make_async_copy(src, dst, small_sem.at[i])
        for i, (src, dst) in enumerate(
            ((bound_in, bound), (extra_in, extra), (mix_in, mix), (scale_in, scale), (gain_in, gain),
             (norm_gain_in, norm_gain), (norm_bias_in, norm_bias)))
    ]

    barrier = pltpu.get_barrier_semaphore()

    @pl.when(tp == 0)
    def _():
        pl.semaphore_signal(barrier, inc=1, device_id={"tp": peer}, device_id_type=MESH)

    n_pairs = heads // 2
    x_in(0).start()
    for copy in fv_in(0, 0):
        copy.start()
    @pl.when(tp > 0)
    def _():
        pl.semaphore_wait(barrier, 1)
        pl.semaphore_signal(met_sem, inc=1, device_id={"tp": peer}, device_id_type=MESH)

    @pl.when(tp == 0)
    def _():
        pl.semaphore_wait(met_sem, 1)

    @pl.when((tp == 0) & (sp > 0))
    def _():
        pl.semaphore_signal(barrier, inc=1, device_id={"sp": lax.rem(sp + n_sp - 1, n_sp)}, device_id_type=MESH)

    for c in range(1, chunks):
        x_in(c).start()
    for pr in range(1, n_pairs):
        for copy in fv_in(pr, 0):
            copy.start()
    for copy in smalls:
        copy.start()

    p_buf[pl.ds(0, BLOCK_ROWS), :] = jnp.zeros((BLOCK_ROWS, pool_w), BF16)
    state[...] = jnp.zeros_like(state)

    row_ids = lax.broadcasted_iota(jnp.int32, (BLOCK_ROWS, BLOCK_ROWS), 0)
    col_ids = lax.broadcasted_iota(jnp.int32, (BLOCK_ROWS, BLOCK_ROWS), 1)
    lower = row_ids >= col_ids
    tri = jnp.where(lower, 1.0, 0.0).astype(BF16)
    tri_twice = jnp.concatenate([tri, tri], axis=1)

    def own_fv(c, pr):
        rows = rows_of(c)
        r_buf[rows, 2 * pr * pair:2 * (pr + 1) * pair] = dot(x_own[rows], fv_buf[pr, 0])

    def peer_fv(c, pr):
        rows = rows_of(c)
        cols = slice(pr * pair, (pr + 1) * pair)
        part = dot(x_peer[rows], fv_buf[pr, 1])
        for i, buf in ((0, f_buf), (1, v_buf)):
            base = (2 * pr + i) * pair
            buf[rows, cols] = (r_buf[rows, base:base + pair] + part[:, i * pair:(i + 1) * pair]).astype(BF16)
        yield

    def project(c, i, buf, base=0):
        rows = rows_of(c)
        part = dot(x_own[rows], w_buf[i, 0])
        yield
        buf[rows_of(c, ROWS, base), :] = (part + dot(x_peer[rows], w_buf[i, 1])).astype(BF16)
        yield

    def gate_one(b, pr):
        brows = rows_of(b, BLOCK_ROWS)
        lanes = slice(pr * pair, (pr + 1) * pair)
        tile = BLOCK_ROWS // 4
        tiles = [slice(b * BLOCK_ROWS + k * tile, b * BLOCK_ROWS + (k + 1) * tile) for k in range(4)]
        weights, highs, lows = [], [], []
        for part in tiles:
            f_in = f_buf[part, lanes].astype(F32)
            drop = jnp.concatenate(
                [jnp.broadcast_to(extra_t[part, h:h + 1], (tile, DK)) for h in (2 * pr, 2 * pr + 1)], axis=1)
            weight = (1.0 - bound[:, lanes]) * (0.5 - 0.5 * jnp.tanh(0.5 * f_in))
            keep = jnp.log(1.0 - weight) + drop
            high = keep.astype(BF16)
            highs.append(high)
            lows.append((keep - high.astype(F32)).astype(BF16))
            e_buf[part, lanes] = weight
        total = dot(tri_twice, jnp.concatenate(highs + lows, axis=0))
        yield
        middle = 0.5 * total[BLOCK_ROWS - 1:BLOCK_ROWS]
        half = jnp.exp(middle)
        half_buf[b, :, lanes] = jnp.broadcast_to(half, (8, pair))
        downs = []
        for k, part in enumerate(tiles):
            apart = total[k * tile:(k + 1) * tile] - middle
            down = (e_buf[part, lanes] * jnp.exp(-apart)).astype(BF16)
            downs.append(down)
            u_buf[part, lanes] = down
            e_buf[part, lanes] = jnp.exp(apart)
        down = jnp.concatenate(downs, axis=0)
        terms = [
            dot(v_buf[brows, pr * pair + j * DK:pr * pair + (j + 1) * DK], down[:, j * DK:(j + 1) * DK], TN)
            for j in range(2)]
        yield
        term = jnp.concatenate(terms, axis=1) * half
        t_buf[b, :, lanes] = term
        state[:, lanes] = half * half * state[:, lanes] + term
        yield

    def gates(c, pr):
        return skew([gate_one(c * per + k, pr) for k in range(per)], 3)

    back = (lax.broadcasted_iota(jnp.int32, (BLOCK_ROWS, 2 * BLOCK_ROWS), 0) + BLOCK_ROWS
            - lax.broadcasted_iota(jnp.int32, (BLOCK_ROWS, 2 * BLOCK_ROWS), 1))
    count = lax.broadcasted_iota(jnp.int32, (BLOCK_ROWS, LANES), 0) + (sp * length + 1)

    def pool_one(b, j):
        start = b * BLOCK_ROWS
        brows = rows_of(b, BLOCK_ROWS)
        lanes = slice(j * GROUP_CH, (j + 1) * GROUP_CH)
        near = p_buf[rows_of(b, BLOCK_ROWS, 0), lanes]
        here = p_buf[rows_of(b, BLOCK_ROWS, BLOCK_ROWS), lanes]
        window = jnp.left_shift(jnp.int32(2), tp * groups + j)
        band = jnp.where((back >= 0) & (back < window), 1.0, 0.0).astype(BF16)
        sums = dot(band, jnp.concatenate([near, here], axis=0))
        yield
        share = 1.0 / jnp.minimum(count + start, window).astype(F32)
        share = jnp.concatenate([share] * (GROUP_CH // LANES), axis=1)
        diff = (sums * share - here.astype(F32)).astype(BF16)
        mixed = dot(diff, mix[j])
        yield
        a_own[brows, lanes] = (mixed * scale[:, lanes]).astype(BF16)
        yield

    def pools(c):
        return skew([pool_one(c * per + k, j) for k in range(per) for j in range(groups)], 3, 2)

    def score_one(b, h):
        brows = rows_of(b, BLOCK_ROWS)
        lanes = slice(h * DK, (h + 1) * DK)
        q_in = q_buf[brows, lanes].astype(F32)
        up = (q_in * half_sigmoid(q_in) * e_buf[brows, lanes]).astype(BF16)
        sq_buf[brows, h * pair + DK:(h + 1) * pair] = up
        tile = dot(up, u_buf[brows, lanes], NT)
        yield
        sq_buf[brows, h * pair:h * pair + DK] = jnp.where(lower, tile, 0.0).astype(BF16)
        yield

    def scores(c):
        return skew([score_one(c * per + k, h) for k in range(per) for h in range(heads)], 2, 3)

    def mix_one(b, h):
        brows = rows_of(b, BLOCK_ROWS)
        lanes = slice(h * DK, (h + 1) * DK)
        half = half_buf[b, 0:1, lanes]
        before = state[:, lanes] * half
        state[:, lanes] = before * half + t_buf[b, :, lanes]
        carried = jnp.transpose(before.astype(BF16))
        yield
        raw = dot(sq_buf[brows, h * pair:(h + 1) * pair],
                  jnp.concatenate([v_buf[brows, lanes], carried], axis=0))
        yield
        power = jnp.mean(raw * raw, axis=-1, keepdims=True)
        yield
        gate = g_buf[brows, lanes].astype(F32)
        rec = raw * lax.rsqrt(power + EPS_RMS) * gain[...] * (gate * half_sigmoid(gate))
        a_own[brows, pool_w + h * DK:pool_w + (h + 1) * DK] = rec.astype(BF16)
        yield

    def mixes(c):
        return skew([mix_one(c * per + k, h) for k in range(per) for h in range(heads)], 4)

    with jax.named_scope("own_fv"):
        x_in(0).wait()
        x_out(0).start()
        for copy in fv_in(0, 0):
            copy.wait()
        own_fv(0, 0)
        for c in range(1, chunks):
            x_in(c).wait()
            x_out(c).start()
        for pr in range(n_pairs):
            for copy in fv_in(pr, 1):
                copy.start()
        for c in range(1, chunks):
            own_fv(c, 0)
        for pr in range(1, n_pairs):
            for copy in fv_in(pr, 0):
                copy.wait()
        for copy in smalls:
            copy.wait()
        for b in range(blocks):
            brows = rows_of(b, BLOCK_ROWS)
            extra_t[brows, 0:heads] = jnp.transpose(extra[:, brows])
        for pr in range(1, n_pairs):
            for c in range(chunks):
                own_fv(c, pr)

    for i in range(3):
        for k in range(n_tp):
            w_in(i, k).start()
    for i in range(2):
        wo_in(i).start()
        wo_out(i).start()

    more = sp + 1 < n_sp

    def own_state(pr):
        @pl.when((sp == 0) & more)
        def _():
            state_out[pr] = state[:, pr * pair:(pr + 1) * pair].astype(BF16)
            st_out(pr).start()

    def next_state(pr, here):
        @pl.when(here & (sp > 0) & more)
        def _():
            lanes = slice(pr * pair, (pr + 1) * pair)
            root = half_buf[0, 0:1, lanes]
            for b in range(1, blocks):
                root = root * half_buf[b, 0:1, lanes]
            st_out(pr).wait_recv()
            state_out[pr] = (root * root * state_in[pr].astype(F32) + state[:, lanes]).astype(BF16)
            st_out(pr).start()

    fv_steps = [(c, pr) for pr in range(heads // 2) for c in range(chunks)]
    gate_items = [gate_one(b, pr) for pr in range(heads // 2) for b in range(blocks)]

    def fv_step(k):
        if k >= len(fv_steps):
            for _ in project(chunks - 1, 0, p_buf, BLOCK_ROWS):
                pass
            return
        c, pr = fv_steps[k]
        if pr == 0 and c % 2 == 0:
            for d in (c, c + 1):
                x_out(d).wait_recv()
        for _ in peer_fv(c, pr):
            pass

    gate_lag = 2

    def gate_slot(t):
        for stage in (2, 1, 0):
            if 0 <= t - gate_lag * stage < len(gate_items):
                next(gate_items[t - gate_lag * stage], None)

    for pr in range(n_pairs):
        for copy in fv_in(pr, 1):
            copy.wait()
    with jax.named_scope("fv"):
        fv_step(0)
        fv_step(1)
        for t in range(blocks + 2 * gate_lag):
            if t % per == 0:
                fv_step(2 + t // per)
            gate_slot(t)

    with jax.named_scope("greet_wait"):
        @pl.when((tp == 0) & more)
        def _():
            pl.semaphore_wait(barrier, 1)
            pl.semaphore_signal(go_sem, inc=1, device_id={"tp": peer}, device_id_type=MESH)

        @pl.when((tp > 0) & more)
        def _():
            pl.semaphore_wait(go_sem, 1)

        own_state(0)

    for k in range(n_tp):
        w_in(0, k).wait()

    with jax.named_scope("fv_next"):
        for t in range(blocks + 2 * gate_lag, 2 * blocks + 2 * gate_lag):
            if t % per == 0 and 2 + t // per <= len(fv_steps):
                fv_step(2 + t // per)
            gate_slot(t)

    with jax.named_scope("sends"):
        @pl.when(more)
        def _():
            h_out(sp + 1).start()

        own_state(1)

    for i in (1, 2):
        for k in range(n_tp):
            w_in(i, k).wait()

    with jax.named_scope("pool_query"):
        for c in range(chunks - 1):
            weave([(2, project(c, 0, p_buf, BLOCK_ROWS))], [])
        next_state(0, sp == 1)
        weave([(2, project(0, 1, q_buf))], [])
        for c in range(1, chunks):
            weave([(2, project(c, 1, q_buf))], [scores(c - 1), pools(c)])
            if c == 1:
                next_state(1, sp == 1)
        for c in range(1, chunks):
            a_out(0, c).start()

    with jax.named_scope("halo_wait"):
        @pl.when(sp > 0)
        def _():
            h_out(sp).wait_recv()
            p_buf[pl.ds(BLOCK_ROWS - HALO, HALO), :] = halo_in[...]

        next_state(0, sp > 1)

    with jax.named_scope("gate0"):
        weave([(2, project(0, 2, g_buf))], [scores(chunks - 1), pools(0)])
        a_out(0, 0).start()
        next_state(1, sp > 1)

    with jax.named_scope("gate"):
        for c in range(1, chunks):
            weave([(2, project(c, 2, g_buf))], [])

    for i in range(2):
        wo_in(i).wait()
        wo_out(i).wait_recv()
    for c in range(chunks):
        a_out(0, c).wait_recv()
    pool_at, rec_at = (place for _, place in wo_places)

    def out_pool(c):
        rows = rows_of(c)
        for n in range(2):
            cols = slice(n * (feats // 2), (n + 1) * (feats // 2))
            r_buf[rows, cols] = (
                dot(a_own[rows, pool_at], wo_own[pool_at, cols])
                + dot(a_peer[rows, pool_at], wo_peer[pool_at, cols]))
            yield

    with jax.named_scope("out_pool0"):
        weave([(2, out_pool(0))], [])

    def first_state(pr):
        lanes = slice(pr * pair, (pr + 1) * pair)

        @pl.when((sp > 0) & (sp + 1 == n_sp))
        def _():
            st_out(pr).wait_recv()

        @pl.when(sp == 0)
        def _():
            state[:, lanes] = jnp.zeros((DK, pair), F32)

        @pl.when(sp > 0)
        def _():
            state[:, lanes] = state_in[pr].astype(F32)

    with jax.named_scope("join"):
        first_state(0)

    mix_items = [
        mix_one(c * per + k, h) for c in range(chunks) for pr in range(n_pairs) for k in range(per)
        for h in (2 * pr, 2 * pr + 1)]
    per_mix = per * heads

    mix_lags = (0, 2, 4, 5)

    def mix_slot(t):
        for stage in (3, 2, 1, 0):
            if 0 <= t - mix_lags[stage] < len(mix_items):
                next(mix_items[t - mix_lags[stage]], None)

    def fold(x):
        acc = x[:, :LANES]
        for k in range(1, x.shape[1] // LANES):
            acc = acc + x[:, k * LANES:(k + 1) * LANES]
        return acc

    first_half = lax.broadcasted_iota(jnp.int32, (32, LANES), 1) < LANES // 2

    def out_one(c, n):
        rows = rows_of(c)
        cols = slice(n * (feats // 2), (n + 1) * (feats // 2))
        full = (dot(a_own[rows, rec_at], wo_own[rec_at, cols])
                + dot(a_peer[rows, rec_at], wo_peer[rec_at, cols]))
        yield
        tile = 32
        for k in range(ROWS // tile):
            part = slice(c * ROWS + k * tile, c * ROWS + (k + 1) * tile)
            here = slice(k * tile, (k + 1) * tile)
            resid = full[here] + (r_buf[part, cols] + ALPHA * x_own[part, cols].astype(F32))
            r_buf[part, cols] = resid
            sums, squares = fold(resid), fold(resid * resid)
            both = jnp.where(first_half, sums + pltpu.roll(sums, LANES // 2, 1),
                             squares + pltpu.roll(squares, LANES // 2, 1))
            stat_own[c, here] = both if n == 0 else stat_own[c, here] + both
        if n == 1:
            s_out(c).start()
        yield

    def norm(c):
        def one(k):
            here = slice(k * 32, (k + 1) * 32)
            both = stat_own[c, here] + stat_peer[c, here]
            mean = jnp.sum(jnp.where(first_half, both, 0.0), axis=1, keepdims=True) / (n_tp * feats)
            square = jnp.sum(jnp.where(first_half, 0.0, both), axis=1, keepdims=True) / (n_tp * feats)
            inv = lax.rsqrt(square - mean * mean + EPS_NORM)
            yield
            part = slice(c * ROWS + k * 32, c * ROWS + (k + 1) * 32)
            for n in range(2):
                cols = slice(n * (feats // 2), (n + 1) * (feats // 2))
                o_buf[part, cols] = (
                    (r_buf[part, cols] - mean) * inv * norm_gain[:, cols] + norm_bias[:, cols]).astype(BF16)
            yield

        for _ in skew([one(k) for k in range(ROWS // 32)], 2, 3)[1]:
            pass
        o_out(c).start()

    def mix_slots(first, last):
        for t in range(first, min(last, len(mix_items) + mix_lags[3])):
            mix_slot(t)
            if t % per_mix == mix_lags[3] - 1 and t >= per_mix:
                a_out(1, t // per_mix - 1).start()

    pieces = [(c, n) for c in range(1, chunks) for n in range(2)]
    per_piece = -(-(len(mix_items) + mix_lags[3]) // (len(pieces) + 1))

    with jax.named_scope("out_pool"):
        for k, (c, n) in enumerate(pieces):
            if n == 0:
                step = out_pool(c)
            next(step, None)
            if k == 0:
                mix_slots(0, per_mix // n_pairs)
                for pr in range(1, n_pairs):
                    first_state(pr)
                mix_slots(per_mix // n_pairs, per_piece)
            else:
                mix_slots(k * per_piece, (k + 1) * per_piece)

    out_items = [out_one(c, n) for c in range(chunks) for n in range(2)]

    def out_slot(k):
        for stage in (0, 1):
            if 0 <= k - stage < len(out_items):
                next(out_items[k - stage], None)

    with jax.named_scope("out0"):
        a_out(1, 0).wait_recv()
        out_slot(0)
        mix_slots(len(pieces) * per_piece, len(mix_items) + mix_lags[3])
        out_slot(1)

    with jax.named_scope("out2"):
        for c in range(1, chunks - 1):
            a_out(1, c).wait_recv()
        for k in range(2, 2 * chunks - 2):
            out_slot(k)

    with jax.named_scope("out3"):
        a_out(1, chunks - 1).wait_recv()
        out_slot(2 * chunks - 2)
        out_slot(2 * chunks - 1)
        for c in range(chunks - 3):
            s_out(c).wait_recv()
            norm(c)
        out_slot(2 * chunks)

    with jax.named_scope("stats"):
        for c in range(chunks - 3, chunks):
            s_out(c).wait_recv()
            norm(c)

    with jax.named_scope("drain"):
        for c in range(chunks):
            x_out(c).wait_send()
            s_out(c).wait_send()
            o_out(c).wait()
            for i in range(2):
                a_out(i, c).wait_send()
        for i in range(2):
            wo_out(i).wait_send()

        @pl.when(more)
        def _():
            for pr in range(heads // 2):
                st_out(pr).wait_send()

        @pl.when(sp + 1 < n_sp)
        def _():
            h_out(sp + 1).wait_send()


def finish(pieces, normed, out, buf, in_sem, out_sem):
    rows = normed.shape[0] // pieces

    def copies(c):
        part = pl.ds(c * rows, rows)
        return (
            pltpu.make_async_copy(normed.at[part], buf.at[part], in_sem.at[c]),
            pltpu.make_async_copy(buf.at[part], out.at[0, part], out_sem.at[c]),
        )

    for c in range(pieces):
        copies(c)[0].start()
    for c in range(pieces):
        copies(c)[0].wait()
        copies(c)[1].start()
    for c in range(pieces):
        copies(c)[1].wait()


def solution(mesh):
    n_sp, n_tp = mesh.shape["sp"], mesh.shape["tp"]

    def local(stream, w_pool, w_query, w_forget, w_value, w_gate, mix, scale, bound, extra,
              gain, wo_pool, wo_rec, norm_gain, norm_bias):
        length, feats = stream.shape[1], stream.shape[2]
        chans, pool_w = bound.shape[0], scale.shape[0]
        blocks = length // BLOCK_ROWS
        chunks = length // ROWS
        pairs = chans // DK // 2
        hbm = pl.BlockSpec(memory_space=pl.ANY)
        dma = pltpu.SemaphoreType.DMA
        scratch = [
            pltpu.VMEM((length, feats), BF16),
            pltpu.VMEM((length, feats), BF16),
            pltpu.VMEM((3, n_tp, feats, chans), BF16),
            pltpu.VMEM((pairs, n_tp, feats, 4 * DK), BF16),
            pltpu.VMEM((pool_w + chans, feats), BF16),
            pltpu.VMEM((pool_w + chans, feats), BF16),
            pltpu.VMEM((length, pool_w + chans), BF16),
            pltpu.VMEM((length, pool_w + chans), BF16),
            pltpu.VMEM((length, chans), BF16),
            pltpu.VMEM((length, chans), BF16),
            pltpu.VMEM((length, chans), BF16),
            pltpu.VMEM((length, chans), F32),
            pltpu.VMEM((blocks, DK, chans), F32),
            pltpu.VMEM((BLOCK_ROWS + length, pool_w), BF16),
            pltpu.VMEM((length, chans), BF16),
            pltpu.VMEM((length, 2 * chans), BF16),
            pltpu.VMEM((length, chans), BF16),
            pltpu.VMEM((length, max(feats, 2 * chans)), F32),
            pltpu.VMEM((length, feats), BF16),
            pltpu.VMEM((blocks, 8, chans), F32),
            pltpu.VMEM((DK, chans), F32),
            pltpu.VMEM((pairs, DK, 2 * DK), BF16),
            pltpu.VMEM((pairs, DK, 2 * DK), BF16),
            pltpu.VMEM((HALO, pool_w), BF16),
            pltpu.VMEM((chunks, ROWS, LANES), F32),
            pltpu.VMEM((chunks, ROWS, LANES), F32),
            pltpu.VMEM((1, feats), F32),
            pltpu.VMEM((1, feats), F32),
            pltpu.VMEM(mix.shape, BF16),
            pltpu.VMEM((1, pool_w), F32),
            pltpu.VMEM((1, chans), F32),
            pltpu.VMEM((chans // DK, length), F32),
            pltpu.VMEM((length, LANES), F32),
            pltpu.VMEM((1, DK), F32),
            dma((chunks,)), dma((chunks,)), dma((chunks,)), dma((3, n_tp)), dma((pairs, n_tp, 2)),
            dma((2,)), dma((2,)), dma((2,)), dma((2, chunks)), dma((2, chunks)),
            dma((pairs,)), dma((pairs,)), dma, dma, dma((chunks,)), dma((chunks,)), dma((chunks,)),
            dma((7,)), pltpu.SemaphoreType.REGULAR, pltpu.SemaphoreType.REGULAR,
        ]
        row = lambda x: x.reshape(1, -1)
        normed = pl.pallas_call(
            functools.partial(mixer, n_sp, n_tp),
            out_shape=jax.ShapeDtypeStruct((length, feats), BF16),
            in_specs=[hbm] * 15,
            out_specs=hbm,
            scratch_shapes=scratch,
            compiler_params=pltpu.CompilerParams(
                collective_id=0, has_side_effects=True, vmem_limit_bytes=60 * 1024 * 1024),
            name="mixer",
        )(stream, w_pool, w_query, w_forget, w_value, w_gate, mix, row(scale), row(bound), extra.T,
          row(gain), wo_pool, wo_rec, row(norm_gain), row(norm_bias))
        pieces = 4
        return pl.pallas_call(
            functools.partial(finish, pieces),
            out_shape=jax.ShapeDtypeStruct(stream.shape, BF16),
            in_specs=[hbm],
            out_specs=hbm,
            scratch_shapes=[pltpu.VMEM((length, feats), BF16), dma((pieces,)), dma((pieces,))],
            compiler_params=pltpu.CompilerParams(vmem_limit_bytes=60 * 1024 * 1024),
            name="finish",
        )(normed)

    placed = (
        P("fs", "sp", "tp"), P(None, "tp"), P(None, "tp"), P(None, "tp"), P(None, "tp"),
        P(None, "tp"), P("tp", None, None), P("tp"), P("tp"), P("sp", "tp"), P(),
        P("tp", None), P("tp", None), P("tp"), P("tp"),
    )
    return jax.shard_map(
        local, mesh=mesh, in_specs=placed, out_specs=P("fs", "sp", "tp"), check_vma=False
    )
```

```python
import functools

import jax
import jax.numpy as jnp
from jax import lax
from jax.experimental import pallas as pl
from jax.experimental.pallas import tpu as pltpu
from jax.sharding import PartitionSpec as P

DK = 128
BLOCK_ROWS = 128
GROUP_CH = 256
HALO = 16
LANES = 128
ROWS = 256

ALPHA = 2.0**0.25
EPS_RMS = 1e-06
EPS_NORM = 1e-05
F32 = jnp.float32
BF16 = jnp.bfloat16
NT = (((1,), (1,)), ((), ()))
TN = (((0,), (0,)), ((), ()))
MESH = pl.DeviceIdType.MESH


def dot(a, b, dims=None):
    if dims is None:
        return jnp.dot(a, b, preferred_element_type=F32)
    return lax.dot_general(a, b, dims, preferred_element_type=F32)


def half_sigmoid(x):
    return 0.5 + 0.5 * jnp.tanh(0.5 * x)


def skew(items, stages, lag=1):
    items, count = list(items), 0
    order = []
    for t in range(len(items) + lag * (stages - 1)):
        for stage in reversed(range(stages)):
            if 0 <= t - stage * lag < len(items):
                order.append(t - stage * lag)
                count += 1

    def run():
        for i in order:
            next(items[i], None)
            yield

    return count, run()


def weave(bigs, smalls):
    n_big, n_small = (sum(n for n, _ in steps) for steps in (bigs, smalls))
    rest = [step for _, steps in smalls for step in [steps]]
    small = (None for steps in rest for _ in steps)
    done = 0
    for i, _ in enumerate(piece for _, steps in bigs for piece in steps):
        want = -(-(i + 1) * n_small // n_big)
        while done < want:
            next(small, None)
            done += 1
    for _ in small:
        pass


def mixer(
    n_sp, n_tp,
    stream, w_pool, w_query, w_forget, w_value, w_gate,
    mix_in, scale_in, bound_in, extra_in, gain_in, wo_pool, wo_rec, norm_gain_in, norm_bias_in,
    out,
    x_own, x_peer, w_buf, fv_buf, wo_own, wo_peer, a_own, a_peer, f_buf, v_buf, u_buf, e_buf, t_buf, p_buf, q_buf, sq_buf, g_buf, r_buf,
    o_buf, half_buf, state, state_out, state_in, halo_in, stat_own, stat_peer, norm_gain, norm_bias,
    mix, scale, bound, extra, extra_t, gain,
    x_loc, x_send, x_recv, w_sem, fv_sem, wo_loc, wo_send, wo_recv, a_send, a_recv,
    st_send, st_recv, h_send, h_recv, s_send, s_recv, o_sem, small_sem, met_sem, go_sem,
):
    sp, tp = lax.axis_index("sp"), lax.axis_index("tp")
    peer = 1 - tp
    length, feats = stream.shape[1], stream.shape[2]
    chans = bound.shape[1]
    heads = chans // DK
    pool_w = scale.shape[1]
    groups = mix.shape[0]
    chunks = length // ROWS
    blocks = length // BLOCK_ROWS
    per = ROWS // BLOCK_ROWS
    pair = 2 * DK

    def rows_of(c, size=ROWS, base=0):
        start = c * size + base
        return pl.ds(start if isinstance(start, int) else pl.multiple_of(start, BLOCK_ROWS), size)

    def x_in(c):
        rows = rows_of(c)
        return pltpu.make_async_copy(stream.at[0, rows], x_own.at[rows], x_loc.at[c])

    def x_out(c):
        rows = rows_of(c)
        return pltpu.make_async_remote_copy(
            x_own.at[rows], x_peer.at[rows], x_send.at[c], x_recv.at[c],
            device_id={"tp": peer}, device_id_type=MESH)

    def w_rows(k):
        return pl.ds(pl.multiple_of((tp, peer)[k] * feats, LANES), feats)

    def w_in(i, k):
        src = (w_pool, w_query, w_gate)[i]
        return pltpu.make_async_copy(src.at[w_rows(k)], w_buf.at[i, k], w_sem.at[i, k])

    def fv_in(pr, k):
        return [
            pltpu.make_async_copy(
                src.at[w_rows(k), pl.ds(pr * pair, pair)], fv_buf.at[pr, k, :, pl.ds(i * pair, pair)],
                fv_sem.at[pr, k, i])
            for i, src in enumerate((w_forget, w_value))]

    my_cols = pl.ds(pl.multiple_of(tp * feats, LANES), feats)
    peer_cols = pl.ds(pl.multiple_of(peer * feats, LANES), feats)
    wo_places = ((wo_pool, pl.ds(0, pool_w)), (wo_rec, pl.ds(pool_w, chans)))

    def wo_in(i):
        src, place = wo_places[i]
        return pltpu.make_async_copy(src.at[:, my_cols], wo_own.at[place], wo_loc.at[i])

    def wo_out(i):
        src, place = wo_places[i]
        return pltpu.make_async_remote_copy(
            src.at[:, peer_cols], wo_peer.at[place], wo_send.at[i], wo_recv.at[i],
            device_id={"tp": peer}, device_id_type=MESH)

    def a_out(i, c):
        rows, cols = rows_of(c), wo_places[i][1]
        return pltpu.make_async_remote_copy(
            a_own.at[rows, cols], a_peer.at[rows, cols], a_send.at[i, c], a_recv.at[i, c],
            device_id={"tp": peer}, device_id_type=MESH)

    def st_out(pr):
        return pltpu.make_async_remote_copy(
            state_out.at[pr], state_in.at[pr], st_send.at[pr], st_recv.at[pr],
            device_id={"sp": lax.rem(sp + 1, n_sp)}, device_id_type=MESH)

    def h_out(k):
        return pltpu.make_async_remote_copy(
            p_buf.at[pl.ds(BLOCK_ROWS + length - HALO, HALO)], halo_in, h_send, h_recv,
            device_id={"sp": k}, device_id_type=MESH)

    def s_out(c):
        return pltpu.make_async_remote_copy(
            stat_own.at[c], stat_peer.at[c], s_send.at[c], s_recv.at[c],
            device_id={"tp": peer}, device_id_type=MESH)

    def o_out(c):
        rows = rows_of(c)
        return pltpu.make_async_copy(o_buf.at[rows], out.at[rows], o_sem.at[c])

    smalls = [
        pltpu.make_async_copy(src, dst, small_sem.at[i])
        for i, (src, dst) in enumerate(
            ((bound_in, bound), (extra_in, extra), (mix_in, mix), (scale_in, scale), (gain_in, gain),
             (norm_gain_in, norm_gain), (norm_bias_in, norm_bias)))
    ]

    barrier = pltpu.get_barrier_semaphore()

    @pl.when(tp == 0)
    def _():
        pl.semaphore_signal(barrier, inc=1, device_id={"tp": peer}, device_id_type=MESH)

    n_pairs = heads // 2
    x_in(0).start()
    for copy in fv_in(0, 0):
        copy.start()
    @pl.when(tp > 0)
    def _():
        pl.semaphore_wait(barrier, 1)
        pl.semaphore_signal(met_sem, inc=1, device_id={"tp": peer}, device_id_type=MESH)

    @pl.when(tp == 0)
    def _():
        pl.semaphore_wait(met_sem, 1)

    @pl.when((tp == 0) & (sp > 0))
    def _():
        pl.semaphore_signal(barrier, inc=1, device_id={"sp": lax.rem(sp + n_sp - 1, n_sp)}, device_id_type=MESH)

    for c in range(1, chunks):
        x_in(c).start()
    for pr in range(1, n_pairs):
        for copy in fv_in(pr, 0):
            copy.start()
    for copy in smalls:
        copy.start()

    p_buf[pl.ds(0, BLOCK_ROWS), :] = jnp.zeros((BLOCK_ROWS, pool_w), BF16)
    state[...] = jnp.zeros_like(state)

    row_ids = lax.broadcasted_iota(jnp.int32, (BLOCK_ROWS, BLOCK_ROWS), 0)
    col_ids = lax.broadcasted_iota(jnp.int32, (BLOCK_ROWS, BLOCK_ROWS), 1)
    lower = row_ids >= col_ids
    tri = jnp.where(lower, 1.0, 0.0).astype(BF16)
    tri_twice = jnp.concatenate([tri, tri], axis=1)

    def own_fv(c, pr):
        rows = rows_of(c)
        r_buf[rows, 2 * pr * pair:2 * (pr + 1) * pair] = dot(x_own[rows], fv_buf[pr, 0])

    def peer_fv(c, pr):
        rows = rows_of(c)
        cols = slice(pr * pair, (pr + 1) * pair)
        part = dot(x_peer[rows], fv_buf[pr, 1])
        for i, buf in ((0, f_buf), (1, v_buf)):
            base = (2 * pr + i) * pair
            buf[rows, cols] = (r_buf[rows, base:base + pair] + part[:, i * pair:(i + 1) * pair]).astype(BF16)
        yield

    def project(c, i, buf, base=0):
        rows = rows_of(c)
        part = dot(x_own[rows], w_buf[i, 0])
        yield
        buf[rows_of(c, ROWS, base), :] = (part + dot(x_peer[rows], w_buf[i, 1])).astype(BF16)
        yield

    def gate_one(b, pr):
        brows = rows_of(b, BLOCK_ROWS)
        lanes = slice(pr * pair, (pr + 1) * pair)
        tile = BLOCK_ROWS // 4
        tiles = [slice(b * BLOCK_ROWS + k * tile, b * BLOCK_ROWS + (k + 1) * tile) for k in range(4)]
        weights, highs, lows = [], [], []
        for part in tiles:
            f_in = f_buf[part, lanes].astype(F32)
            drop = jnp.concatenate(
                [jnp.broadcast_to(extra_t[part, h:h + 1], (tile, DK)) for h in (2 * pr, 2 * pr + 1)], axis=1)
            weight = (1.0 - bound[:, lanes]) * (0.5 - 0.5 * jnp.tanh(0.5 * f_in))
            keep = jnp.log(1.0 - weight) + drop
            high = keep.astype(BF16)
            highs.append(high)
            lows.append((keep - high.astype(F32)).astype(BF16))
            e_buf[part, lanes] = weight
        total = dot(tri_twice, jnp.concatenate(highs + lows, axis=0))
        yield
        middle = 0.5 * total[BLOCK_ROWS - 1:BLOCK_ROWS]
        half = jnp.exp(middle)
        half_buf[b, :, lanes] = jnp.broadcast_to(half, (8, pair))
        downs = []
        for k, part in enumerate(tiles):
            apart = total[k * tile:(k + 1) * tile] - middle
            down = (e_buf[part, lanes] * jnp.exp(-apart)).astype(BF16)
            downs.append(down)
            u_buf[part, lanes] = down
            e_buf[part, lanes] = jnp.exp(apart)
        down = jnp.concatenate(downs, axis=0)
        terms = [
            dot(v_buf[brows, pr * pair + j * DK:pr * pair + (j + 1) * DK], down[:, j * DK:(j + 1) * DK], TN)
            for j in range(2)]
        yield
        term = jnp.concatenate(terms, axis=1) * half
        t_buf[b, :, lanes] = term
        state[:, lanes] = half * half * state[:, lanes] + term
        yield

    def gates(c, pr):
        return skew([gate_one(c * per + k, pr) for k in range(per)], 3)

    back = (lax.broadcasted_iota(jnp.int32, (BLOCK_ROWS, 2 * BLOCK_ROWS), 0) + BLOCK_ROWS
            - lax.broadcasted_iota(jnp.int32, (BLOCK_ROWS, 2 * BLOCK_ROWS), 1))
    count = lax.broadcasted_iota(jnp.int32, (BLOCK_ROWS, LANES), 0) + (sp * length + 1)

    def pool_one(b, j):
        start = b * BLOCK_ROWS
        brows = rows_of(b, BLOCK_ROWS)
        lanes = slice(j * GROUP_CH, (j + 1) * GROUP_CH)
        near = p_buf[rows_of(b, BLOCK_ROWS, 0), lanes]
        here = p_buf[rows_of(b, BLOCK_ROWS, BLOCK_ROWS), lanes]
        window = jnp.left_shift(jnp.int32(2), tp * groups + j)
        band = jnp.where((back >= 0) & (back < window), 1.0, 0.0).astype(BF16)
        sums = dot(band, jnp.concatenate([near, here], axis=0))
        yield
        share = 1.0 / jnp.minimum(count + start, window).astype(F32)
        share = jnp.concatenate([share] * (GROUP_CH // LANES), axis=1)
        diff = (sums * share - here.astype(F32)).astype(BF16)
        mixed = dot(diff, mix[j])
        yield
        a_own[brows, lanes] = (mixed * scale[:, lanes]).astype(BF16)
        yield

    def pools(c):
        return skew([pool_one(c * per + k, j) for k in range(per) for j in range(groups)], 3, 2)

    def score_one(b, h):
        brows = rows_of(b, BLOCK_ROWS)
        lanes = slice(h * DK, (h + 1) * DK)
        q_in = q_buf[brows, lanes].astype(F32)
        up = (q_in * half_sigmoid(q_in) * e_buf[brows, lanes]).astype(BF16)
        sq_buf[brows, h * pair + DK:(h + 1) * pair] = up
        tile = dot(up, u_buf[brows, lanes], NT)
        yield
        sq_buf[brows, h * pair:h * pair + DK] = jnp.where(lower, tile, 0.0).astype(BF16)
        yield

    def scores(c):
        return skew([score_one(c * per + k, h) for k in range(per) for h in range(heads)], 2, 3)

    def mix_one(b, h):
        brows = rows_of(b, BLOCK_ROWS)
        lanes = slice(h * DK, (h + 1) * DK)
        half = half_buf[b, 0:1, lanes]
        before = state[:, lanes] * half
        state[:, lanes] = before * half + t_buf[b, :, lanes]
        carried = jnp.transpose(before.astype(BF16))
        yield
        raw = dot(sq_buf[brows, h * pair:(h + 1) * pair],
                  jnp.concatenate([v_buf[brows, lanes], carried], axis=0))
        yield
        power = jnp.mean(raw * raw, axis=-1, keepdims=True)
        yield
        gate = g_buf[brows, lanes].astype(F32)
        rec = raw * lax.rsqrt(power + EPS_RMS) * gain[...] * (gate * half_sigmoid(gate))
        a_own[brows, pool_w + h * DK:pool_w + (h + 1) * DK] = rec.astype(BF16)
        yield

    def mixes(c):
        return skew([mix_one(c * per + k, h) for k in range(per) for h in range(heads)], 4)

    with jax.named_scope("own_fv"):
        x_in(0).wait()
        x_out(0).start()
        for copy in fv_in(0, 0):
            copy.wait()
        own_fv(0, 0)
        for c in range(1, chunks):
            x_in(c).wait()
            x_out(c).start()
        for pr in range(n_pairs):
            for copy in fv_in(pr, 1):
                copy.start()
        for c in range(1, chunks):
            own_fv(c, 0)
        for pr in range(1, n_pairs):
            for copy in fv_in(pr, 0):
                copy.wait()
        for copy in smalls:
            copy.wait()
        for b in range(blocks):
            brows = rows_of(b, BLOCK_ROWS)
            extra_t[brows, 0:heads] = jnp.transpose(extra[:, brows])
        for pr in range(1, n_pairs):
            for c in range(chunks):
                own_fv(c, pr)

    for i in range(3):
        for k in range(n_tp):
            w_in(i, k).start()
    for i in range(2):
        wo_in(i).start()
        wo_out(i).start()

    more = sp + 1 < n_sp

    def own_state(pr):
        @pl.when((sp == 0) & more)
        def _():
            state_out[pr] = state[:, pr * pair:(pr + 1) * pair].astype(BF16)
            st_out(pr).start()

    def next_state(pr, here):
        @pl.when(here & (sp > 0) & more)
        def _():
            lanes = slice(pr * pair, (pr + 1) * pair)
            root = half_buf[0, 0:1, lanes]
            for b in range(1, blocks):
                root = root * half_buf[b, 0:1, lanes]
            st_out(pr).wait_recv()
            state_out[pr] = (root * root * state_in[pr].astype(F32) + state[:, lanes]).astype(BF16)
            st_out(pr).start()

    fv_steps = [(c, pr) for pr in range(heads // 2) for c in range(chunks)]
    gate_items = [gate_one(b, pr) for pr in range(heads // 2) for b in range(blocks)]

    def fv_step(k):
        if k >= len(fv_steps):
            for _ in project(chunks - 1, 0, p_buf, BLOCK_ROWS):
                pass
            return
        c, pr = fv_steps[k]
        if pr == 0 and c % 2 == 0:
            for d in (c, c + 1):
                x_out(d).wait_recv()
        for _ in peer_fv(c, pr):
            pass

    gate_lag = 2

    def gate_slot(t):
        for stage in (0, 2, 1):
            if 0 <= t - gate_lag * stage < len(gate_items):
                next(gate_items[t - gate_lag * stage], None)

    for pr in range(n_pairs):
        for copy in fv_in(pr, 1):
            copy.wait()
    with jax.named_scope("fv"):
        fv_step(0)
        fv_step(1)
        for t in range(blocks + 2 * gate_lag):
            if t % per == 0:
                fv_step(2 + t // per)
            gate_slot(t)

    with jax.named_scope("greet_wait"):
        @pl.when((tp == 0) & more)
        def _():
            pl.semaphore_wait(barrier, 1)
            pl.semaphore_signal(go_sem, inc=1, device_id={"tp": peer}, device_id_type=MESH)

        @pl.when((tp > 0) & more)
        def _():
            pl.semaphore_wait(go_sem, 1)

        own_state(0)

    for k in range(n_tp):
        w_in(0, k).wait()

    with jax.named_scope("fv_next"):
        for t in range(blocks + 2 * gate_lag, 2 * blocks + 2 * gate_lag):
            if t % per == 0 and 2 + t // per <= len(fv_steps):
                fv_step(2 + t // per)
            gate_slot(t)

    with jax.named_scope("sends"):
        @pl.when(more)
        def _():
            h_out(sp + 1).start()

        own_state(1)

    for i in (1, 2):
        for k in range(n_tp):
            w_in(i, k).wait()

    with jax.named_scope("pool_query"):
        for c in range(chunks - 1):
            weave([(2, project(c, 0, p_buf, BLOCK_ROWS))], [])
        next_state(0, sp == 1)
        weave([(2, project(0, 1, q_buf))], [])
        for c in range(1, chunks):
            weave([(2, project(c, 1, q_buf))], [scores(c - 1), pools(c)])
            if c == 1:
                next_state(1, sp == 1)
        for c in range(1, chunks):
            a_out(0, c).start()

    with jax.named_scope("halo_wait"):
        @pl.when(sp > 0)
        def _():
            h_out(sp).wait_recv()
            p_buf[pl.ds(BLOCK_ROWS - HALO, HALO), :] = halo_in[...]

        next_state(0, sp > 1)

    with jax.named_scope("gate0"):
        weave([(2, project(0, 2, g_buf))], [scores(chunks - 1), pools(0)])
        a_out(0, 0).start()
        next_state(1, sp > 1)

    with jax.named_scope("gate"):
        for c in range(1, chunks):
            weave([(2, project(c, 2, g_buf))], [])

    for i in range(2):
        wo_in(i).wait()
        wo_out(i).wait_recv()
    for c in range(chunks):
        a_out(0, c).wait_recv()
    pool_at, rec_at = (place for _, place in wo_places)

    def out_pool(c):
        rows = rows_of(c)
        for n in range(2):
            cols = slice(n * (feats // 2), (n + 1) * (feats // 2))
            r_buf[rows, cols] = (
                dot(a_own[rows, pool_at], wo_own[pool_at, cols])
                + dot(a_peer[rows, pool_at], wo_peer[pool_at, cols]))
            yield

    with jax.named_scope("out_pool0"):
        weave([(2, out_pool(0))], [])

    def first_state(pr):
        lanes = slice(pr * pair, (pr + 1) * pair)

        @pl.when((sp > 0) & (sp + 1 == n_sp))
        def _():
            st_out(pr).wait_recv()

        @pl.when(sp == 0)
        def _():
            state[:, lanes] = jnp.zeros((DK, pair), F32)

        @pl.when(sp > 0)
        def _():
            state[:, lanes] = state_in[pr].astype(F32)

    with jax.named_scope("join"):
        first_state(0)

    mix_items = [
        mix_one(c * per + k, h) for c in range(chunks) for pr in range(n_pairs) for k in range(per)
        for h in (2 * pr, 2 * pr + 1)]
    per_mix = per * heads

    mix_lags = (0, 2, 5, 7)

    def mix_slot(t):
        for stage in (3, 2, 1, 0):
            if 0 <= t - mix_lags[stage] < len(mix_items):
                next(mix_items[t - mix_lags[stage]], None)

    def fold(x):
        acc = x[:, :LANES]
        for k in range(1, x.shape[1] // LANES):
            acc = acc + x[:, k * LANES:(k + 1) * LANES]
        return acc

    first_half = lax.broadcasted_iota(jnp.int32, (32, LANES), 1) < LANES // 2

    def out_one(c, n):
        rows = rows_of(c)
        cols = slice(n * (feats // 2), (n + 1) * (feats // 2))
        full = (dot(a_own[rows, rec_at], wo_own[rec_at, cols])
                + dot(a_peer[rows, rec_at], wo_peer[rec_at, cols]))
        yield
        tile = 32
        for k in range(ROWS // tile):
            part = slice(c * ROWS + k * tile, c * ROWS + (k + 1) * tile)
            here = slice(k * tile, (k + 1) * tile)
            resid = full[here] + (r_buf[part, cols] + ALPHA * x_own[part, cols].astype(F32))
            r_buf[part, cols] = resid
            sums, squares = fold(resid), fold(resid * resid)
            both = jnp.where(first_half, sums + pltpu.roll(sums, LANES // 2, 1),
                             squares + pltpu.roll(squares, LANES // 2, 1))
            stat_own[c, here] = both if n == 0 else stat_own[c, here] + both
        if n == 1:
            s_out(c).start()
        yield

    def norm(c):
        def one(k):
            here = slice(k * 32, (k + 1) * 32)
            both = stat_own[c, here] + stat_peer[c, here]
            mean = jnp.sum(jnp.where(first_half, both, 0.0), axis=1, keepdims=True) / (n_tp * feats)
            square = jnp.sum(jnp.where(first_half, 0.0, both), axis=1, keepdims=True) / (n_tp * feats)
            inv = lax.rsqrt(square - mean * mean + EPS_NORM)
            yield
            part = slice(c * ROWS + k * 32, c * ROWS + (k + 1) * 32)
            for n in range(2):
                cols = slice(n * (feats // 2), (n + 1) * (feats // 2))
                o_buf[part, cols] = (
                    (r_buf[part, cols] - mean) * inv * norm_gain[:, cols] + norm_bias[:, cols]).astype(BF16)
            yield

        for _ in skew([one(k) for k in range(ROWS // 32)], 2, 3)[1]:
            pass
        o_out(c).start()

    def mix_slots(first, last):
        for t in range(first, min(last, len(mix_items) + mix_lags[3])):
            mix_slot(t)
            if t % per_mix == mix_lags[3] - 1 and t >= per_mix:
                a_out(1, t // per_mix - 1).start()

    pieces = [(c, n) for c in range(1, chunks) for n in range(2)]
    per_piece = -(-(len(mix_items) + mix_lags[3]) // (len(pieces) + 1))

    with jax.named_scope("out_pool"):
        for k, (c, n) in enumerate(pieces):
            if n == 0:
                step = out_pool(c)
            next(step, None)
            if k == 0:
                mix_slots(0, per_mix // n_pairs)
                for pr in range(1, n_pairs):
                    first_state(pr)
                mix_slots(per_mix // n_pairs, per_piece)
            else:
                mix_slots(k * per_piece, (k + 1) * per_piece)

    out_items = [out_one(c, n) for c in range(chunks) for n in range(2)]

    def out_slot(k):
        for stage in (0, 1):
            if 0 <= k - stage < len(out_items):
                next(out_items[k - stage], None)

    with jax.named_scope("out0"):
        a_out(1, 0).wait_recv()
        out_slot(0)
        mix_slots(len(pieces) * per_piece, len(mix_items) + mix_lags[3])
        out_slot(1)

    with jax.named_scope("out2"):
        for c in range(1, chunks - 1):
            a_out(1, c).wait_recv()
        for k in range(2, 2 * chunks - 2):
            out_slot(k)

    with jax.named_scope("out3"):
        a_out(1, chunks - 1).wait_recv()
        out_slot(2 * chunks - 2)
        out_slot(2 * chunks - 1)
        out_slot(2 * chunks)
        for c in range(chunks - 3):
            s_out(c).wait_recv()
            norm(c)

    with jax.named_scope("stats"):
        for c in range(chunks - 3, chunks):
            s_out(c).wait_recv()
            norm(c)

    with jax.named_scope("drain"):
        for c in range(chunks):
            x_out(c).wait_send()
            s_out(c).wait_send()
            o_out(c).wait()
            for i in range(2):
                a_out(i, c).wait_send()
        for i in range(2):
            wo_out(i).wait_send()

        @pl.when(more)
        def _():
            for pr in range(heads // 2):
                st_out(pr).wait_send()

        @pl.when(sp + 1 < n_sp)
        def _():
            h_out(sp + 1).wait_send()


def finish(pieces, normed, out, buf, in_sem, out_sem):
    rows = normed.shape[0] // pieces

    def copies(c):
        part = pl.ds(c * rows, rows)
        return (
            pltpu.make_async_copy(normed.at[part], buf.at[part], in_sem.at[c]),
            pltpu.make_async_copy(buf.at[part], out.at[0, part], out_sem.at[c]),
        )

    for c in range(pieces):
        copies(c)[0].start()
    for c in range(pieces):
        copies(c)[0].wait()
        copies(c)[1].start()
    for c in range(pieces):
        copies(c)[1].wait()


def solution(mesh):
    n_sp, n_tp = mesh.shape["sp"], mesh.shape["tp"]

    def local(stream, w_pool, w_query, w_forget, w_value, w_gate, mix, scale, bound, extra,
              gain, wo_pool, wo_rec, norm_gain, norm_bias):
        length, feats = stream.shape[1], stream.shape[2]
        chans, pool_w = bound.shape[0], scale.shape[0]
        blocks = length // BLOCK_ROWS
        chunks = length // ROWS
        pairs = chans // DK // 2
        hbm = pl.BlockSpec(memory_space=pl.ANY)
        dma = pltpu.SemaphoreType.DMA
        scratch = [
            pltpu.VMEM((length, feats), BF16),
            pltpu.VMEM((length, feats), BF16),
            pltpu.VMEM((3, n_tp, feats, chans), BF16),
            pltpu.VMEM((pairs, n_tp, feats, 4 * DK), BF16),
            pltpu.VMEM((pool_w + chans, feats), BF16),
            pltpu.VMEM((pool_w + chans, feats), BF16),
            pltpu.VMEM((length, pool_w + chans), BF16),
            pltpu.VMEM((length, pool_w + chans), BF16),
            pltpu.VMEM((length, chans), BF16),
            pltpu.VMEM((length, chans), BF16),
            pltpu.VMEM((length, chans), BF16),
            pltpu.VMEM((length, chans), F32),
            pltpu.VMEM((blocks, DK, chans), F32),
            pltpu.VMEM((BLOCK_ROWS + length, pool_w), BF16),
            pltpu.VMEM((length, chans), BF16),
            pltpu.VMEM((length, 2 * chans), BF16),
            pltpu.VMEM((length, chans), BF16),
            pltpu.VMEM((length, max(feats, 2 * chans)), F32),
            pltpu.VMEM((length, feats), BF16),
            pltpu.VMEM((blocks, 8, chans), F32),
            pltpu.VMEM((DK, chans), F32),
            pltpu.VMEM((pairs, DK, 2 * DK), BF16),
            pltpu.VMEM((pairs, DK, 2 * DK), BF16),
            pltpu.VMEM((HALO, pool_w), BF16),
            pltpu.VMEM((chunks, ROWS, LANES), F32),
            pltpu.VMEM((chunks, ROWS, LANES), F32),
            pltpu.VMEM((1, feats), F32),
            pltpu.VMEM((1, feats), F32),
            pltpu.VMEM(mix.shape, BF16),
            pltpu.VMEM((1, pool_w), F32),
            pltpu.VMEM((1, chans), F32),
            pltpu.VMEM((chans // DK, length), F32),
            pltpu.VMEM((length, LANES), F32),
            pltpu.VMEM((1, DK), F32),
            dma((chunks,)), dma((chunks,)), dma((chunks,)), dma((3, n_tp)), dma((pairs, n_tp, 2)),
            dma((2,)), dma((2,)), dma((2,)), dma((2, chunks)), dma((2, chunks)),
            dma((pairs,)), dma((pairs,)), dma, dma, dma((chunks,)), dma((chunks,)), dma((chunks,)),
            dma((7,)), pltpu.SemaphoreType.REGULAR, pltpu.SemaphoreType.REGULAR,
        ]
        row = lambda x: x.reshape(1, -1)
        normed = pl.pallas_call(
            functools.partial(mixer, n_sp, n_tp),
            out_shape=jax.ShapeDtypeStruct((length, feats), BF16),
            in_specs=[hbm] * 15,
            out_specs=hbm,
            scratch_shapes=scratch,
            compiler_params=pltpu.CompilerParams(
                collective_id=0, has_side_effects=True, vmem_limit_bytes=60 * 1024 * 1024),
            name="mixer",
        )(stream, w_pool, w_query, w_forget, w_value, w_gate, mix, row(scale), row(bound), extra.T,
          row(gain), wo_pool, wo_rec, row(norm_gain), row(norm_bias))
        pieces = 4
        return pl.pallas_call(
            functools.partial(finish, pieces),
            out_shape=jax.ShapeDtypeStruct(stream.shape, BF16),
            in_specs=[hbm],
            out_specs=hbm,
            scratch_shapes=[pltpu.VMEM((length, feats), BF16), dma((pieces,)), dma((pieces,))],
            compiler_params=pltpu.CompilerParams(vmem_limit_bytes=60 * 1024 * 1024),
            name="finish",
        )(normed)

    placed = (
        P("fs", "sp", "tp"), P(None, "tp"), P(None, "tp"), P(None, "tp"), P(None, "tp"),
        P(None, "tp"), P("tp", None, None), P("tp"), P("tp"), P("sp", "tp"), P(),
        P("tp", None), P("tp", None), P("tp"), P("tp"),
    )
    return jax.shard_map(
        local, mesh=mesh, in_specs=placed, out_specs=P("fs", "sp", "tp"), check_vma=False
    )
```
